32 devices in a mesh: sp: 8 (over z, x), tp: 4 (over y, core).
Axes of the slice: x: 2, y: 2, z: 4, core: 2. Of those that a mesh axis runs over, the one named last changes fastest.
Arguments:
- x_in: bfloat16 [8, 3072, 2048], P('tp', 'sp'), may hold values from -13 to 13
- x_new: bfloat16 [8, 2048], P('sp'), may hold values from -6 to 6
- w_x: bfloat16 [2048, 2048], replicated, may hold values from -0.125 to 0.125
- w_b: bfloat16 [2048, 1024], replicated, may hold values from -0.125 to 0.125
- w_c: bfloat16 [2048, 1024], replicated, may hold values from -0.125 to 0.125
- w_dt: bfloat16 [2048, 32], replicated, may hold values from -0.125 to 0.125
- w_z: bfloat16 [2048, 2048], P(None, 'tp'), may hold values from -3 to 3
- conv_w: float32 [4, 4096], replicated, may hold values from -3 to 3
- conv_b: float32 [4096], replicated, may hold values from -3 to 3
- dt_bias: float32 [32], replicated, may hold values from -4 to -2
- a_log: float32 [32], replicated, may hold values from -12 to 0
- d_skip: float32 [32], replicated, may hold values from 1 to 8
- norm_g: float32 [32, 64], P('tp'), may hold values from 0.1 to 1.9
Outputs:
- state_cache: bfloat16 [8, 32, 64, 128], P('sp', 'tp')
- read_out: bfloat16 [8, 32, 64], P('sp', 'tp')
The draws below stay inside these ranges and needn't reach their ends.
All inputs are finite; a program needn't handle non-finite values.
Results may differ from the reference program's by a relative error of at most 0.015.
Values may be sent and summed in bfloat16 or wider, within the bound.
A program may use at most 128 MiB of HBM per device.

```python
import math
import jax
import jax.numpy as jnp
from jax import lax

D = 2048
H = 32
P_SIZE = 64
G = 8
N = 128
KW = 4
POS_DEV = 384
R = 4
SEQS = 8
LENGTH = 3072


def draw_x_in(key, part):
    normal_key, factor_key = jax.random.split(key)
    blocks = LENGTH // POS_DEV
    factor = jnp.exp(jax.random.uniform(factor_key, (SEQS, blocks, 1), jnp.float32, -1.2, 1.2))
    factor = jnp.repeat(factor, POS_DEV, axis=1)
    values = jnp.clip(jax.random.normal(normal_key, (SEQS, LENGTH, D), jnp.float32), -3.9, 3.9) * factor
    return values.astype(jnp.bfloat16)


def draw_a_log(key, part):
    pick_key, fast_key, slow_key = jax.random.split(key, 3)
    pick_draw = jax.random.uniform(pick_key, (H,), jnp.float32)
    fast_share = 0.5
    fast_mag = jnp.exp(jax.random.uniform(fast_key, (H,), jnp.float32, math.log(0.15), math.log(0.5)))
    slow_mag = jnp.exp(jax.random.uniform(slow_key, (H,), jnp.float32, math.log(5.0 / LENGTH), math.log(15.0 / LENGTH)))
    return jnp.log(jnp.where(pick_draw < fast_share, fast_mag, slow_mag)).astype(jnp.float32)


def draw_w_z(key, part):
    entry_key, scale_key = jax.random.split(key)
    col_scale = jnp.exp(jax.random.uniform(scale_key, (1, H * P_SIZE), jnp.float32, -1.2, 1.2))
    entries = jnp.clip(jax.random.normal(entry_key, (D, H * P_SIZE), jnp.float32), -6.0, 6.0)
    return (entries * col_scale * D ** (-0.5)).astype(jnp.bfloat16)


def level_of(key, extent, cuts, least, largest):
    factor_of = 1.0
    for dim, blocks in cuts:
        draws = jax.random.uniform(jax.random.fold_in(jax.random.fold_in(key, 6), dim), (blocks,), jnp.float32, least / len(cuts), largest / len(cuts))
        factor_of = factor_of * jnp.repeat(jnp.exp(draws), extent[dim] // blocks).reshape((-1,) + (1,) * (len(extent) - 1 - dim))
    return factor_of


def noise(rng, dims, width, limit, shards=(), dtype=jnp.bfloat16):
    factor_of = level_of(rng, dims, shards, -0.22, 0.18) if shards else 1.0
    array = jax.random.normal(rng, dims, jnp.float32) * width * factor_of
    return jnp.minimum(jnp.maximum(array, -limit), limit).astype(dtype)


def setup_inputs(seed: int = 0) -> dict:
    key_of = jax.random.split(jax.random.key(seed), 14)
    x_in = draw_x_in(jax.random.fold_in(key_of[13], 71), 0)
    x_new = noise(key_of[1], (SEQS, D), 1.0, 6.0, ((0, 8),))
    w_x = noise(key_of[2], (D, H * P_SIZE), D ** -0.5, 0.125)
    w_b = noise(key_of[3], (D, G * N), D ** -0.5, 0.125)
    w_c = noise(key_of[4], (D, G * N), D ** -0.5, 0.125)
    w_dt = noise(key_of[5], (D, H), D ** -0.5, 0.125)
    w_z = draw_w_z(jax.random.fold_in(key_of[13], 71), 0)
    conv_w = noise(key_of[7], (KW, H * P_SIZE + 2 * G * N), 0.5, 3.0, (), jnp.float32)
    conv_b = noise(key_of[8], (H * P_SIZE + 2 * G * N,), 0.5, 3.0, (), jnp.float32)
    dt_bias = jnp.clip(jax.random.uniform(key_of[9], (H,), jnp.float32, -4.0, -2.0), -4.0, -2.0)
    a_log = draw_a_log(jax.random.fold_in(key_of[13], 71), 0)
    d_skip = jnp.clip(jnp.exp(jax.random.uniform(key_of[11], (H,), jnp.float32, math.log(1.0), math.log(8.0))), 1.0, 8.0)
    norm_g = jnp.clip(1.0 + 0.18 * jax.random.normal(key_of[12], (H, P_SIZE), jnp.float32), 0.1, 1.9)
    return {"x_in": x_in, "x_new": x_new, "w_x": w_x, "w_b": w_b, "w_c": w_c, "w_dt": w_dt, "w_z": w_z, "conv_w": conv_w, "conv_b": conv_b, "dt_bias": dt_bias, "a_log": a_log, "d_skip": d_skip, "norm_g": norm_g}


eps = 1e-05

def shift_conv(padded, weights, biases, col_count):
    acc_sum = biases + jnp.zeros(padded.shape[:1] + (col_count,) + padded.shape[2:], jnp.float32)
    for offset in range(KW):
        acc_sum = acc_sum + weights[offset] * padded[:, offset:offset + col_count].astype(jnp.float32)
    return jax.nn.silu(acc_sum).astype(jnp.bfloat16)

def reference(x_in, x_new, w_x, w_b, w_c, w_dt, w_z, conv_w, conv_b, dt_bias, a_log, d_skip, norm_g):
    inner_cols = H * P_SIZE
    state_cols = G * N
    edge_rows = KW - 1
    decay_rates = -jnp.exp(a_log)

    def one_sequence(token_rows):
        pre_values = jnp.dot(token_rows, w_x, preferred_element_type=jnp.float32).astype(jnp.bfloat16)
        pre_keys = jnp.dot(token_rows, w_b, preferred_element_type=jnp.float32).astype(jnp.bfloat16)
        raw_steps = jnp.dot(token_rows, w_dt, preferred_element_type=jnp.float32).astype(jnp.bfloat16)
        joined = jnp.concatenate([pre_values, pre_keys], axis=1)
        padded = jnp.concatenate([jnp.zeros((edge_rows, joined.shape[1]), jnp.bfloat16), joined], axis=0)
        conved = shift_conv(padded[None], conv_w[:, :inner_cols + state_cols], conv_b[:inner_cols + state_cols], LENGTH)[0]
        step_sizes = jax.nn.softplus(raw_steps.astype(jnp.float32) + dt_bias)
        rest_sum = lax.cumsum(step_sizes, axis=0, reverse=True) - step_sizes
        weight = jnp.exp(decay_rates * rest_sum) * step_sizes
        scaled = (weight[:, :, None] * conved[:, :inner_cols].astype(jnp.float32).reshape(LENGTH, H, P_SIZE)).astype(jnp.bfloat16)
        key_rows = conved[:, inner_cols:].astype(jnp.float32).reshape(LENGTH, G, N)
        state = jnp.einsum('lgrp,lgn->grpn', scaled.astype(jnp.float32).reshape(LENGTH, G, R, P_SIZE), key_rows, precision=lax.Precision.HIGHEST).reshape(H, P_SIZE, N)
        pre_query = jnp.dot(token_rows[LENGTH - edge_rows:], w_c, preferred_element_type=jnp.float32).astype(jnp.bfloat16)
        tail_rows = jnp.concatenate([joined[LENGTH - edge_rows:], pre_query], axis=1)
        return (state, tail_rows)
    states, tails = lax.map(one_sequence, x_in)
    new_pre = jnp.concatenate([jnp.dot(x_new, w_x, preferred_element_type=jnp.float32).astype(jnp.bfloat16), jnp.dot(x_new, w_b, preferred_element_type=jnp.float32).astype(jnp.bfloat16), jnp.dot(x_new, w_c, preferred_element_type=jnp.float32).astype(jnp.bfloat16)], axis=1)
    new_raw = jnp.dot(x_new, w_dt, preferred_element_type=jnp.float32).astype(jnp.bfloat16)
    gate_new = jnp.dot(x_new, w_z, preferred_element_type=jnp.float32).astype(jnp.bfloat16)
    padded = jnp.concatenate([tails, new_pre[:, None, :]], axis=1)
    new_conv = shift_conv(padded, conv_w, conv_b, 1)[:, 0]
    new_values = new_conv[:, :inner_cols].astype(jnp.float32).reshape(SEQS, G, R, P_SIZE)
    new_keys = new_conv[:, inner_cols:inner_cols + state_cols].astype(jnp.float32).reshape(SEQS, G, N)
    new_query = new_conv[:, inner_cols + state_cols:].astype(jnp.float32).reshape(SEQS, G, N)
    new_steps = jax.nn.softplus(new_raw.astype(jnp.float32) + dt_bias)
    decay_new = jnp.exp(decay_rates * new_steps).reshape(SEQS, G, R)
    held_read = jnp.einsum('sgrpn,sgn->sgrp', states.reshape(SEQS, G, R, P_SIZE, N), new_query, precision=lax.Precision.HIGHEST)
    inner_prod = lax.optimization_barrier(jnp.sum(new_query * new_keys, axis=-1))
    step_group = new_steps.reshape(SEQS, G, R)
    output = decay_new[..., None] * held_read + (step_group * inner_prod[:, :, None])[..., None] * new_values + d_skip.reshape(G, R)[None, :, :, None] * new_values
    gated_out = output * jax.nn.silu(gate_new.astype(jnp.float32).reshape(SEQS, G, R, P_SIZE))
    group_ms = lax.optimization_barrier(jnp.mean(gated_out * gated_out, axis=(2, 3)))
    read_out = gated_out * lax.rsqrt(group_ms + eps)[:, :, None, None] * norm_g.reshape(G, R, P_SIZE)
    return (states.astype(jnp.bfloat16), read_out.astype(jnp.bfloat16).reshape(SEQS, H, P_SIZE))
```

```python
import functools

import jax
import jax.numpy as jnp
from jax import lax
from jax.experimental import pallas as pl
from jax.experimental.pallas import tpu as pltpu
from jax.sharding import PartitionSpec as P

MESH = pl.DeviceIdType.MESH
F32 = jnp.float32
BF16 = jnp.bfloat16
EPS = 1e-05
EDGE = 16
PAIR = 2
LANES = 128


def silu(x):
    half = 0.5 * x
    return half + half * jnp.tanh(half)


def softplus(x):
    return jnp.maximum(x, 0.0) + jnp.log1p(jnp.exp(-jnp.abs(x)))


def rounded(x):
    return x.astype(BF16).astype(F32)


def kernel(
    dims,
    x_ref, xn_ref, wx_ref, wb_ref, wc_ref, wdt_ref, wz_ref,
    cw_ref, cb_ref, dtb_ref, alog_ref, dskip_ref, ng_ref,
    state_ref, read_ref,
    xs, wxs, wbs, wdts, wxn, wbn, wcn, wzn, nt, pre0, pre1, padded,
    wt, tot_out, tot_in, rate_s, st_out, st_in, head_s, read_s,
    x_sem, wdt_sem, w_sem, new_sem, halo_send, halo_recv, tail_send, tail_recv,
    tot_send, tot_recv, st_send, st_recv,
):
    sp, tp, heads, groups, n_size, p_size, ratio, taps = dims
    i, j = lax.axis_index("sp"), lax.axis_index("tp")
    spt, length, _ = x_ref.shape
    hl, gl = heads // tp, groups // tp
    inner, keys_all = heads * p_size, groups * n_size
    gcols = ratio * p_size
    steps = groups // PAIR
    home = i // spt
    own = home == j
    pres = (pre0, pre1)

    barrier = pltpu.get_barrier_semaphore()
    for k in range(sp):
        @pl.when(jnp.logical_not(own & (i == k)))
        def _():
            pl.semaphore_signal(barrier, inc=1, device_id={"sp": k, "tp": home}, device_id_type=MESH)
    before, after = lax.rem(i + sp - 1, sp), lax.rem(i + 1, sp)
    pl.semaphore_signal(barrier, inc=1, device_id={"sp": before, "tp": j}, device_id_type=MESH)

    wdt_copy = pltpu.make_async_copy(wdt_ref, wdts, wdt_sem)
    x_copies = [
        pltpu.make_async_copy(x_ref.at[a], xs.at[a, pl.ds(EDGE, length)], x_sem.at[a])
        for a in range(spt)
    ]
    w_copies = []
    for s in range(steps):
        w_copies.append((
            pltpu.make_async_copy(
                wx_ref.at[:, pl.ds(s * PAIR * gcols, PAIR * gcols)], wxs.at[s], w_sem.at[s, 0]),
            pltpu.make_async_copy(
                wb_ref.at[:, pl.ds(s * PAIR * n_size, PAIR * n_size)], wbs.at[s], w_sem.at[s, 1]),
        ))
    vcol = pl.multiple_of(j * (hl * p_size), LANES)
    gcol = pl.multiple_of(j * (gl * n_size), LANES)
    new_copies = [
        pltpu.make_async_copy(wx_ref.at[:, pl.ds(vcol, hl * p_size)], wxn, new_sem.at[0]),
        pltpu.make_async_copy(wb_ref.at[:, pl.ds(gcol, gl * n_size)], wbn, new_sem.at[1]),
        pltpu.make_async_copy(wc_ref.at[:, pl.ds(gcol, gl * n_size)], wcn, new_sem.at[2]),
        pltpu.make_async_copy(wz_ref, wzn, new_sem.at[3]),
    ]
    wdt_copy.start()
    for c in x_copies:
        c.start()
    for pair in w_copies:
        for c in pair:
            c.start()
    for c in new_copies:
        c.start()

    pl.semaphore_wait(barrier, spt * tp + 1 - own.astype(jnp.int32))

    def halo(a):
        return pltpu.make_async_remote_copy(
            src_ref=x_ref.at[a, pl.ds(length - EDGE, EDGE)],
            dst_ref=xs.at[a, pl.ds(0, EDGE)],
            send_sem=halo_send.at[a], recv_sem=halo_recv.at[a],
            device_id={"sp": after, "tp": j}, device_id_type=MESH)

    for a in range(spt):
        halo(a).start()

    def is_self(a, q):
        return (spt * j + a == i) & (j == q)

    def either(a, q, remote, local):
        here = is_self(a, q)
        pl.when(jnp.logical_not(here))(remote)
        if local is not None:
            pl.when(here)(local)

    def tail(a, q):
        src, dst = x_ref.at[a, pl.ds(length - EDGE, EDGE)], nt.at[pl.ds(0, EDGE)]
        return pltpu.make_async_remote_copy(
            src_ref=src, dst_ref=dst, send_sem=tail_send.at[a, q], recv_sem=tail_recv.at[0],
            device_id={"sp": spt * j + a, "tp": q}, device_id_type=MESH
        ), pltpu.make_async_copy(src, dst, tail_recv.at[0])

    @pl.when(i == sp - 1)
    def _():
        for a in range(spt):
            for q in range(tp):
                remote, local = tail(a, q)
                either(a, q, remote.start, local.start)

    padded[...] = jnp.zeros_like(padded)
    padded[0:1, 0:heads] = alog_ref[...]
    spread = jnp.broadcast_to(padded[0:1, :], (LANES, LANES)).T[0:heads]
    rates = -jnp.exp(spread)
    for q in range(tp):
        rate_s[q] = rates[q * hl:(q + 1) * hl]
    padded[0:1, 0:heads] = jnp.zeros((1, heads), F32)

    rows = lax.broadcasted_iota(jnp.int32, (length, length), 0)
    cols = lax.broadcasted_iota(jnp.int32, (length, length), 1)
    later = (rows > cols).astype(F32).astype(BF16)
    wdt_copy.wait()

    def tot(a, q):
        src, dst = tot_out.at[a, q], tot_in.at[i]
        return pltpu.make_async_remote_copy(
            src_ref=src, dst_ref=dst, send_sem=tot_send.at[a, q], recv_sem=tot_recv.at[i],
            device_id={"sp": spt * j + a, "tp": q}, device_id_type=MESH
        ), pltpu.make_async_copy(src, dst, tot_recv.at[i])

    for a in range(spt):
        x_copies[a].wait()
        raw = jnp.dot(xs[a, EDGE:, :], wdts[...], preferred_element_type=F32)
        padded[:, 0:heads] = softplus(rounded(raw) + dtb_ref[...])
        sizes = padded[...].T[0:heads]
        rest = jnp.zeros_like(sizes)
        left = sizes
        for _ in range(3):
            term = left.astype(BF16)
            rest += jnp.dot(term, later, preferred_element_type=F32)
            left = left - term.astype(F32)
        wt[a] = jnp.exp(rates[:, 0:1] * rest) * sizes
        total = jnp.broadcast_to(rest[:, 0:1] + sizes[:, 0:1], (heads, LANES))
        for q in range(tp):
            tot_out[a, q] = total[q * hl:(q + 1) * hl]
    for a in range(spt):
        for q in range(tp):
            remote, local = tot(a, q)
            either(a, q, remote.start, local.start)

    for a in range(spt):
        halo(a).wait()
        xs[a, 0:EDGE, :] = jnp.where(i == 0, 0.0, xs[a, 0:EDGE, :].astype(F32)).astype(BF16)

    def state_copy(a, g):
        q = g // gl
        src, dst = st_out.at[a, g], st_in.at[i, lax.rem(g, gl)]
        sem = st_recv.at[i, lax.rem(g, gl)]
        return q, pltpu.make_async_remote_copy(
            src_ref=src, dst_ref=dst, send_sem=st_send.at[a, g], recv_sem=sem,
            device_id={"sp": spt * j + a, "tp": q}, device_id_type=MESH
        ), pltpu.make_async_copy(src, dst, sem)

    vtiles, ktiles = PAIR * gcols // LANES, PAIR * n_size // LANES
    tiles_group = gcols // LANES
    heads_tile = LANES // p_size

    def step(s, carry):
        pltpu.make_async_copy(wx_ref.at[:, pl.ds(0, PAIR * gcols)], wxs.at[s], w_sem.at[s, 0]).wait()
        pltpu.make_async_copy(wb_ref.at[:, pl.ds(0, PAIR * n_size)], wbs.at[s], w_sem.at[s, 1]).wait()

        def project(a):
            values = jnp.dot(xs[a], wxs[s], preferred_element_type=F32)
            for c in range(vtiles):
                pres[a % 2][c] = rounded(values[:, c * LANES:(c + 1) * LANES])
            keys = jnp.dot(xs[a], wbs[s], preferred_element_type=F32)
            for c in range(ktiles):
                pres[a % 2][vtiles + c] = rounded(keys[:, c * LANES:(c + 1) * LANES])

        def conv(a, c):
            if c < vtiles:
                at = pl.multiple_of(s * (PAIR * gcols) + c * LANES, LANES)
            else:
                at = pl.multiple_of(inner + s * (PAIR * n_size) + (c - vtiles) * LANES, LANES)
            acc = cb_ref[:, pl.ds(at, LANES)]
            w = cw_ref[:, pl.ds(at, LANES)]
            for o in range(taps):
                acc = acc + w[o:o + 1] * pres[a % 2][c, pl.ds(EDGE - taps + 1 + o, length), :]
            return silu(acc).astype(BF16)

        def contract(a):
            weights = wt[a, pl.ds(pl.multiple_of(s * (PAIR * ratio), PAIR * ratio), PAIR * ratio), :]
            for gp in range(PAIR):
                key = conv(a, vtiles + gp)
                parts = []
                for c in range(gp * tiles_group, (gp + 1) * tiles_group):
                    turned = conv(a, c).T
                    for r in range(heads_tile):
                        h = c * heads_tile + r
                        part = turned[r * p_size:(r + 1) * p_size].astype(F32)
                        parts.append((weights[h:h + 1] * part).astype(BF16))
                scaled = jnp.concatenate(parts, axis=0)
                g = s * PAIR + gp
                st_out[a, g] = jnp.dot(scaled, key, preferred_element_type=F32).astype(BF16)

        def send(a):
            for gp in range(PAIR):
                q, remote, local = state_copy(a, s * PAIR + gp)
                either(a, q, remote.start, local.start)

        for a in range(spt):
            project(a)
            if a > 0:
                contract(a - 1)
        contract(spt - 1)
        for a in range(spt):
            send(a)
        return carry

    lax.fori_loop(0, steps, step, 0)

    newest = jnp.broadcast_to(xn_ref[...].astype(F32), (EDGE, xn_ref.shape[1])).astype(BF16)
    nt[EDGE:2 * EDGE, :] = newest
    tail(0, 0)[0].wait_recv()
    for c in new_copies:
        c.wait()

    def new_conv(w_ref, start, width):
        pre = rounded(jnp.dot(nt[...], w_ref[...], preferred_element_type=F32))
        start = pl.multiple_of(start, LANES)
        acc = cb_ref[:, pl.ds(start, width)]
        w = cw_ref[:, pl.ds(start, width)]
        for o in range(taps):
            at = EDGE - taps + 1 + o
            acc = acc + w[o:o + 1] * pre[at:at + 1]
        return rounded(silu(acc))

    new_values = new_conv(wxn, vcol, hl * p_size)
    new_keys = new_conv(wbn, inner + gcol, gl * n_size)
    new_query = new_conv(wcn, inner + keys_all + gcol, gl * n_size)
    gate = rounded(jnp.dot(newest, wzn[...], preferred_element_type=F32)[0:1])
    new_raw = rounded(jnp.dot(newest, wdts[...], preferred_element_type=F32)[0:1])
    new_steps = softplus(new_raw + dtb_ref[...])
    head_s[...] = jnp.zeros_like(head_s)
    head_s[0:1, :] = new_steps
    head_s[1:2, :] = jnp.exp(-jnp.exp(alog_ref[...]) * new_steps)
    head_s[2:3, :] = dskip_ref[...]
    hrow = lax.broadcasted_iota(jnp.int32, (heads, hl * p_size), 0)
    hcol = lax.broadcasted_iota(jnp.int32, (heads, hl * p_size), 1)
    first = j * hl
    onehot = ((hcol >= (hrow - first) * p_size) & (hcol < (hrow - first + 1) * p_size)).astype(F32)
    spread_rows = jnp.dot(head_s[...], onehot, precision=lax.Precision.HIGHEST, preferred_element_type=F32)
    step_row, decay_row, skip_row = spread_rows[0:1], spread_rows[1:2], spread_rows[2:3]

    for k in range(sp):
        pltpu.make_async_remote_copy(
            src_ref=tot_out.at[0, 0], dst_ref=tot_in.at[k], send_sem=tot_send.at[0, 0],
            recv_sem=tot_recv.at[k], device_id={"sp": after, "tp": j}, device_id_type=MESH).wait_recv()
    rate_local = rate_s[j]
    factors = [None] * sp
    later_sum = jnp.zeros((hl, LANES), F32)
    for k in reversed(range(sp)):
        factors[k] = jnp.exp(rate_local * later_sum)
        later_sum = later_sum + tot_in[k]
    for g in range(gl):
        for k in range(sp):
            pltpu.make_async_remote_copy(
                src_ref=st_out.at[0, 0], dst_ref=st_in.at[k, g], send_sem=st_send.at[0, 0],
                recv_sem=st_recv.at[k, g], device_id={"sp": after, "tp": j}, device_id_type=MESH).wait_recv()
        query = new_query[:, g * n_size:(g + 1) * n_size]
        key = new_keys[:, g * n_size:(g + 1) * n_size]
        query_rows = jnp.broadcast_to(query, (EDGE, n_size)).astype(BF16)
        helds = []
        for r in range(ratio):
            h = g * ratio + r
            acc = jnp.zeros((p_size, n_size), F32)
            for k in range(sp):
                acc += factors[k][h:h + 1] * st_in[k, g, r * p_size:(r + 1) * p_size, :].astype(F32)
            top = acc.astype(BF16)
            state_ref[0, h] = top
            held = jnp.zeros((EDGE, p_size), F32)
            rest = acc
            for _ in range(3):
                term = rest.astype(BF16)
                held += lax.dot_general(query_rows, term, (((1,), (1,)), ((), ())), preferred_element_type=F32)
                rest = rest - term.astype(F32)
            helds.append(held[0:1])
        span = slice(g * gcols, (g + 1) * gcols)
        held_row = jnp.concatenate(helds, axis=1)
        inner_prod = jnp.sum(query * key, axis=1, keepdims=True)
        value_row = new_values[:, span]
        out = (decay_row[:, span] * held_row + (step_row[:, span] * inner_prod) * value_row
               + skip_row[:, span] * value_row)
        gated = out * silu(gate[:, span])
        ms = jnp.sum(gated * gated, axis=1, keepdims=True) / gcols
        normed = gated * lax.rsqrt(ms + EPS)
        for r in range(ratio):
            h = g * ratio + r
            read_s[h:h + 1, :] = normed[:, r * p_size:(r + 1) * p_size] * ng_ref[h:h + 1, :]
    read_ref[0] = read_s[...].astype(BF16)

    @pl.when(i == sp - 1)
    def _():
        for a in range(spt):
            for q in range(tp):
                either(a, q, tail(a, q)[0].wait_send, None)
    for a in range(spt):
        for q in range(tp):
            either(a, q, tot(a, q)[0].wait_send, None)
        for g in range(groups):
            q, remote, _ = state_copy(a, g)
            either(a, q, remote.wait_send, None)


def per_device(
    dims, x_in, x_new, w_x, w_b, w_c, w_dt, w_z, conv_w, conv_b, dt_bias, a_log, d_skip, norm_g
):
    sp, tp, heads, groups, n_size, p_size, ratio, taps = dims
    spt, length, width = x_in.shape
    hl, gl = heads // tp, groups // tp
    assert x_new.shape[0] == 1 and sp == spt * tp and spt <= 2
    steps, gcols = groups // PAIR, ratio * p_size
    tiles = PAIR * (gcols + n_size) // LANES
    any_spec = pl.BlockSpec(memory_space=pl.ANY)
    vmem = pl.BlockSpec(memory_space=pltpu.VMEM)
    dma = pltpu.SemaphoreType.DMA
    return pl.pallas_call(
        functools.partial(kernel, dims),
        out_shape=(
            jax.ShapeDtypeStruct((1, hl, p_size, n_size), BF16),
            jax.ShapeDtypeStruct((1, hl, p_size), BF16),
        ),
        in_specs=[any_spec, vmem] + [any_spec] * 5 + [vmem] * 6,
        out_specs=(vmem, vmem),
        scratch_shapes=[
            pltpu.VMEM((spt, EDGE + length, width), BF16),
            pltpu.VMEM((steps, width, PAIR * gcols), BF16),
            pltpu.VMEM((steps, width, PAIR * n_size), BF16),
            pltpu.VMEM((width, heads), BF16),
            pltpu.VMEM((width, hl * p_size), BF16),
            pltpu.VMEM((width, gl * n_size), BF16),
            pltpu.VMEM((width, gl * n_size), BF16),
            pltpu.VMEM((width, hl * p_size), BF16),
            pltpu.VMEM((2 * EDGE, width), BF16),
            pltpu.VMEM((tiles, EDGE + length, LANES), F32),
            pltpu.VMEM((tiles, EDGE + length, LANES), F32),
            pltpu.VMEM((length, LANES), F32),
            pltpu.VMEM((spt, heads, length), F32),
            pltpu.VMEM((spt, tp, hl, LANES), F32),
            pltpu.VMEM((sp, hl, LANES), F32),
            pltpu.VMEM((tp, hl, LANES), F32),
            pltpu.VMEM((spt, groups, gcols, n_size), BF16),
            pltpu.VMEM((sp, gl, gcols, n_size), BF16),
            pltpu.VMEM((8, heads), F32),
            pltpu.VMEM((hl, p_size), F32),
            dma((spt,)), dma, dma((steps, 2)), dma((4,)), dma((spt,)), dma((spt,)),
            dma((spt, tp)), dma((1,)), dma((spt, tp)), dma((sp,)), dma((spt, groups)), dma((sp, gl)),
        ],
        compiler_params=pltpu.CompilerParams(
            collective_id=0, has_side_effects=True, vmem_limit_bytes=60 * 1024 * 1024
        ),
    )(
        x_in, x_new, w_x, w_b, w_c, w_dt, w_z, conv_w, conv_b.reshape(1, -1),
        dt_bias.reshape(1, -1), a_log.reshape(1, -1), d_skip.reshape(1, -1), norm_g,
    )


def solution(mesh):
    sp, tp = mesh.shape["sp"], mesh.shape["tp"]

    def step(x_in, x_new, w_x, w_b, w_c, w_dt, w_z, conv_w, conv_b, dt_bias, a_log, d_skip, norm_g):
        heads, p_size = w_dt.shape[1], norm_g.shape[1]
        keys_all = w_b.shape[1]
        n_size = LANES
        groups = keys_all // n_size
        dims = (sp, tp, heads, groups, n_size, p_size, heads // groups, conv_w.shape[0])
        return per_device(
            dims, x_in, x_new, w_x, w_b, w_c, w_dt, w_z, conv_w, conv_b, dt_bias, a_log, d_skip, norm_g)

    return jax.shard_map(
        step,
        mesh=mesh,
        in_specs=(
            P("tp", "sp", None), P("sp", None), P(), P(), P(), P(), P(None, "tp"),
            P(), P(), P(), P(), P(), P("tp", None),
        ),
        out_specs=(P("sp", "tp", None, None), P("sp", "tp", None)),
        check_vma=False,
    )
```

```python
import functools

import jax
import jax.numpy as jnp
from jax import lax
from jax.experimental import pallas as pl
from jax.experimental.pallas import tpu as pltpu
from jax.sharding import PartitionSpec as P

MESH = pl.DeviceIdType.MESH
F32 = jnp.float32
BF16 = jnp.bfloat16
EPS = 1e-05
EDGE = 16
PAIR = 2
LANES = 128


def silu(x):
    half = 0.5 * x
    return half + half * jnp.tanh(half)


def softplus(x):
    return jnp.maximum(x, 0.0) + jnp.log1p(jnp.exp(-jnp.abs(x)))


def rounded(x):
    return x.astype(BF16).astype(F32)


def kernel(
    dims,
    x_ref, xn_ref, wx_ref, wb_ref, wc_ref, wdt_ref, wz_ref,
    cw_hbm, cb_hbm, dtb_ref, alog_ref, dskip_ref, ng_ref,
    state_ref, read_ref,
    xs, wxs, wbs, wdts, wxn, wbn, wcn, wzn, nt, pre0, pre1, padded,
    wt, tot_out, tot_in, a_out, a_in, mine, b_in, st_out, st_in, head_s, read_s, cw_ref, cb_ref,
    x_sem, wdt_sem, w_sem, new_sem, conv_sem, halo_send, halo_recv, tail_send, tail_recv,
    tot_send, tot_recv, a_send, a_recv, b_send, b_recv, st_send, st_recv,
):
    sp, tp, heads, groups, n_size, p_size, ratio, taps = dims
    i, j = lax.axis_index("sp"), lax.axis_index("tp")
    spt, length, _ = x_ref.shape
    hl, gl = heads // tp, groups // tp
    inner, keys_all = heads * p_size, groups * n_size
    gcols = ratio * p_size
    steps = groups // PAIR
    home = i // spt
    pres = (pre0, pre1)
    member, m = lax.rem(i, 2), i // 2
    direct = m // 2 == j // 2
    near = jnp.logical_not(direct) & ((j > m) == (lax.rem(m, 2) == 1))
    far = jnp.logical_not(direct) & jnp.logical_not(near)
    partner, sibling = i + 1 - 2 * member, i + 2 - 4 * lax.rem(m, 2)
    pairs = sp // 4

    barrier = pltpu.get_barrier_semaphore()
    for k in range(sp):
        @pl.when(i != k)
        def _():
            pl.semaphore_signal(barrier, inc=1, device_id={"sp": k, "tp": j}, device_id_type=MESH)

        @pl.when(home != j)
        def _():
            pl.semaphore_signal(barrier, inc=1, device_id={"sp": k, "tp": home}, device_id_type=MESH)
    after = lax.rem(i + 1, sp)

    wdt_copy = pltpu.make_async_copy(wdt_ref, wdts, wdt_sem)
    x_copies = [
        pltpu.make_async_copy(x_ref.at[a], xs.at[a, pl.ds(EDGE, length)], x_sem.at[a])
        for a in range(spt)
    ]
    w_copies = []
    for s in range(steps):
        w_copies.append((
            pltpu.make_async_copy(
                wx_ref.at[:, pl.ds(s * PAIR * gcols, PAIR * gcols)], wxs.at[s], w_sem.at[s, 0]),
            pltpu.make_async_copy(
                wb_ref.at[:, pl.ds(s * PAIR * n_size, PAIR * n_size)], wbs.at[s], w_sem.at[s, 1]),
        ))
    vcol = pl.multiple_of(j * (hl * p_size), LANES)
    gcol = pl.multiple_of(j * (gl * n_size), LANES)
    new_copies = [
        pltpu.make_async_copy(wx_ref.at[:, pl.ds(vcol, hl * p_size)], wxn, new_sem.at[0]),
        pltpu.make_async_copy(wb_ref.at[:, pl.ds(gcol, gl * n_size)], wbn, new_sem.at[1]),
        pltpu.make_async_copy(wc_ref.at[:, pl.ds(gcol, gl * n_size)], wcn, new_sem.at[2]),
        pltpu.make_async_copy(wz_ref, wzn, new_sem.at[3]),
    ]
    conv_copies = [
        pltpu.make_async_copy(cw_hbm, cw_ref, conv_sem.at[0]),
        pltpu.make_async_copy(cb_hbm, cb_ref, conv_sem.at[1]),
    ]
    wdt_copy.start()
    for c in x_copies:
        c.start()
    for pair in w_copies[:1]:
        for c in pair:
            c.start()
    for c in conv_copies:
        c.start()
    for pair in w_copies[1:]:
        for c in pair:
            c.start()
    for c in new_copies:
        c.start()

    pl.semaphore_wait(barrier, sp - 1 + spt * (tp - 1))

    def halo(a):
        return pltpu.make_async_remote_copy(
            src_ref=x_ref.at[a, pl.ds(length - EDGE, EDGE)],
            dst_ref=xs.at[a, pl.ds(0, EDGE)],
            send_sem=halo_send.at[a], recv_sem=halo_recv.at[a],
            device_id={"sp": after, "tp": j}, device_id_type=MESH)

    for a in range(spt):
        halo(a).start()

    def is_self(a, q):
        return (spt * j + a == i) & (j == q)

    def either(a, q, remote, local):
        here = is_self(a, q)
        pl.when(jnp.logical_not(here))(remote)
        if local is not None:
            pl.when(here)(local)

    def tail(a, q):
        src, dst = x_ref.at[a, pl.ds(length - EDGE, EDGE)], nt.at[pl.ds(0, EDGE)]
        return pltpu.make_async_remote_copy(
            src_ref=src, dst_ref=dst, send_sem=tail_send.at[a, q], recv_sem=tail_recv.at[0],
            device_id={"sp": spt * j + a, "tp": q}, device_id_type=MESH
        ), pltpu.make_async_copy(src, dst, tail_recv.at[0])

    @pl.when(i == sp - 1)
    def _():
        for a in range(spt):
            for q in range(tp):
                remote, local = tail(a, q)
                either(a, q, remote.start, local.start)

    padded[...] = jnp.zeros_like(padded)

    def column(row):
        padded[0:1, 0:heads] = row
        return jnp.broadcast_to(padded[0:1, :], (LANES, LANES)).T[0:heads]

    rate_row = -jnp.exp(alog_ref[...])
    rates = column(rate_row)

    rows = lax.broadcasted_iota(jnp.int32, (length, length), 0)
    cols = lax.broadcasted_iota(jnp.int32, (length, length), 1)
    later = (rows > cols).astype(F32).astype(BF16)
    wdt_copy.wait()

    def tot(k):
        return pltpu.make_async_remote_copy(
            src_ref=tot_out, dst_ref=tot_in.at[i], send_sem=tot_send.at[k], recv_sem=tot_recv.at[i],
            device_id={"sp": k, "tp": j}, device_id_type=MESH)

    tot_out[...] = jnp.zeros_like(tot_out)
    for a in range(spt):
        x_copies[a].wait()
        raw = lax.dot_general(
            xs[a, EDGE:, :], wdts[...], (((1,), (1,)), ((), ())), preferred_element_type=F32)
        padded[:, 0:heads] = softplus(rounded(raw) + dtb_ref[...])
        tot_out[a:a + 1, :] = jnp.sum(padded[...], axis=0, keepdims=True)
        sizes = padded[...].T[0:heads]
        rest = jnp.zeros_like(sizes)
        left = sizes
        for _ in range(3):
            term = left.astype(BF16)
            rest += jnp.dot(term, later, preferred_element_type=F32)
            left = left - term.astype(F32)
        wt[a] = jnp.exp(rates[:, 0:1] * rest) * sizes
    tot_in[i] = tot_out[...]
    for k in range(sp):
        pl.when(i != k)(tot(k).start)

    for a in range(spt):
        halo(a).wait()
        xs[a, 0:EDGE, :] = jnp.where(i == 0, 0.0, xs[a, 0:EDGE, :].astype(F32)).astype(BF16)

    for k in range(sp):
        @pl.when(i != k)
        def _():
            pltpu.make_async_remote_copy(
                src_ref=tot_out, dst_ref=tot_in.at[k], send_sem=tot_send.at[k], recv_sem=tot_recv.at[k],
                device_id={"sp": k, "tp": j}, device_id_type=MESH).wait_recv()
    beyond = jnp.zeros(tot_out.shape, F32)
    for k in range(sp):
        beyond = beyond + jnp.where(k > i, tot_in[k], 0.0)
    for a in range(spt):
        wt[a] = wt[a] * column(jnp.exp(rate_row * beyond[a:a + 1, 0:heads]))[:, 0:1]

    def a_copy(s):
        return pltpu.make_async_remote_copy(
            src_ref=a_out.at[s], dst_ref=a_in.at[s], send_sem=a_send.at[s], recv_sem=a_recv.at[s],
            device_id={"sp": partner, "tp": j}, device_id_type=MESH)

    def b_copy(s):
        return pltpu.make_async_remote_copy(
            src_ref=st_out.at[s], dst_ref=b_in.at[s], send_sem=b_send.at[s], recv_sem=b_recv.at[s],
            device_id={"sp": sibling, "tp": j}, device_id_type=MESH)

    slot = jnp.where(direct & (lax.rem(m, 2) == 1), pairs, m // 2)

    def state_copy(s, gp):
        g = s * PAIR + gp
        q = g // gl
        src, dst = st_out.at[s, gp], st_in.at[slot, lax.rem(g, gl)]
        sem = st_recv.at[slot, lax.rem(g, gl)]
        return (m == j) & (q == j), pltpu.make_async_remote_copy(
            src_ref=src, dst_ref=dst, send_sem=st_send.at[s, gp], recv_sem=sem,
            device_id={"sp": spt * j + member, "tp": q}, device_id_type=MESH
        ), pltpu.make_async_copy(src, dst, sem)

    def pass_on(s):
        a_copy(s).wait_recv()

        def add(*more):
            for gp in range(PAIR):
                for r in range(0, gcols, LANES):
                    total = mine[s, gp, r:r + LANES, :].astype(F32)
                    for ref in more:
                        total += ref[s, gp, r:r + LANES, :].astype(F32)
                    st_out[s, gp, r:r + LANES, :] = total.astype(BF16)

        @pl.when(near)
        def _():
            b_copy(s).wait_recv()
            add(a_in, b_in)

        @pl.when(jnp.logical_not(near))
        def _():
            add(a_in)

        @pl.when(far)
        def _():
            b_copy(s).start()

        @pl.when(jnp.logical_not(far))
        def _():
            for gp in range(PAIR):
                here, remote, local = state_copy(s, gp)
                pl.when(jnp.logical_not(here))(remote.start)
                pl.when(here)(local.start)

    lag = jnp.where(near, 2, 1)
    for c in conv_copies:
        c.wait()

    vtiles, ktiles = PAIR * gcols // LANES, PAIR * n_size // LANES
    tiles_group = gcols // LANES
    heads_tile = LANES // p_size

    def step(s, carry):
        pltpu.make_async_copy(wx_ref.at[:, pl.ds(0, PAIR * gcols)], wxs.at[s], w_sem.at[s, 0]).wait()
        pltpu.make_async_copy(wb_ref.at[:, pl.ds(0, PAIR * n_size)], wbs.at[s], w_sem.at[s, 1]).wait()

        def project(a):
            values = jnp.dot(xs[a], wxs[s], preferred_element_type=F32)
            for c in range(vtiles):
                pres[a % 2][c] = rounded(values[:, c * LANES:(c + 1) * LANES])
            keys = jnp.dot(xs[a], wbs[s], preferred_element_type=F32)
            for c in range(ktiles):
                pres[a % 2][vtiles + c] = rounded(keys[:, c * LANES:(c + 1) * LANES])

        def conv(a, c):
            if c < vtiles:
                at = pl.multiple_of(s * (PAIR * gcols) + c * LANES, LANES)
            else:
                at = pl.multiple_of(inner + s * (PAIR * n_size) + (c - vtiles) * LANES, LANES)
            acc = cb_ref[:, pl.ds(at, LANES)]
            w = cw_ref[:, pl.ds(at, LANES)]
            for o in range(taps):
                acc = acc + w[o:o + 1] * pres[a % 2][c, pl.ds(EDGE - taps + 1 + o, length), :]
            return silu(acc).astype(BF16)

        def contract(a):
            weights = wt[a, pl.ds(pl.multiple_of(s * (PAIR * ratio), PAIR * ratio), PAIR * ratio), :]
            for gp in range(PAIR):
                key = conv(a, vtiles + gp)
                parts = []
                for c in range(gp * tiles_group, (gp + 1) * tiles_group):
                    turned = conv(a, c).T
                    for r in range(heads_tile):
                        h = c * heads_tile + r
                        part = turned[r * p_size:(r + 1) * p_size].astype(F32)
                        parts.append((weights[h:h + 1] * part).astype(BF16))
                scaled = jnp.concatenate(parts, axis=0)
                term = jnp.dot(scaled, key, preferred_element_type=F32)
                terms[a].append(term.astype(BF16))

        terms = [[] for _ in range(spt)]
        for a in range(spt):
            project(a)
            if a > 0:
                contract(a - 1)
        contract(spt - 1)
        for gp in range(PAIR):
            first, second = (terms[a][gp].astype(F32) for a in range(2))
            a_out[s, gp] = jnp.where(member == 0, second, first).astype(BF16)
            mine[s, gp] = jnp.where(member == 0, first, second).astype(BF16)
        a_copy(s).start()
        pl.when(s >= lag)(lambda: pass_on(s - lag))
        return carry

    lax.fori_loop(0, steps, step, 0)
    pass_on(steps - lag)
    pl.when(near)(lambda: pass_on(steps - 1))

    newest = jnp.broadcast_to(xn_ref[...].astype(F32), (EDGE, xn_ref.shape[1])).astype(BF16)
    nt[EDGE:2 * EDGE, :] = newest
    tail(0, 0)[0].wait_recv()
    for c in new_copies:
        c.wait()

    def new_conv(w_ref, start, width):
        pre = rounded(jnp.dot(nt[...], w_ref[...], preferred_element_type=F32))
        start = pl.multiple_of(start, LANES)
        acc = cb_ref[:, pl.ds(start, width)]
        w = cw_ref[:, pl.ds(start, width)]
        for o in range(taps):
            at = EDGE - taps + 1 + o
            acc = acc + w[o:o + 1] * pre[at:at + 1]
        return rounded(silu(acc))

    new_values = new_conv(wxn, vcol, hl * p_size)
    new_keys = new_conv(wbn, inner + gcol, gl * n_size)
    new_query = new_conv(wcn, inner + keys_all + gcol, gl * n_size)
    gate = rounded(jnp.dot(newest, wzn[...], preferred_element_type=F32)[0:1])
    new_raw = rounded(lax.dot_general(
        newest, wdts[...], (((1,), (1,)), ((), ())), preferred_element_type=F32)[0:1])
    new_steps = softplus(new_raw + dtb_ref[...])
    head_s[...] = jnp.zeros_like(head_s)
    head_s[0:1, :] = new_steps
    head_s[1:2, :] = jnp.exp(-jnp.exp(alog_ref[...]) * new_steps)
    head_s[2:3, :] = dskip_ref[...]
    hrow = lax.broadcasted_iota(jnp.int32, (heads, hl * p_size), 0)
    hcol = lax.broadcasted_iota(jnp.int32, (heads, hl * p_size), 1)
    first = j * hl
    onehot = ((hcol >= (hrow - first) * p_size) & (hcol < (hrow - first + 1) * p_size)).astype(F32)
    spread_rows = jnp.dot(head_s[...], onehot, precision=lax.Precision.HIGHEST, preferred_element_type=F32)
    step_row, decay_row, skip_row = spread_rows[0:1], spread_rows[1:2], spread_rows[2:3]

    for g in range(gl):
        for k in range(pairs + 1):
            pltpu.make_async_remote_copy(
                src_ref=st_out.at[0, 0], dst_ref=st_in.at[k, g], send_sem=st_send.at[0, 0],
                recv_sem=st_recv.at[k, g], device_id={"sp": after, "tp": j}, device_id_type=MESH).wait_recv()
        query = new_query[:, g * n_size:(g + 1) * n_size]
        key = new_keys[:, g * n_size:(g + 1) * n_size]
        query_rows = jnp.broadcast_to(query, (EDGE, n_size)).astype(BF16)
        helds = []
        for r in range(ratio):
            h = g * ratio + r
            acc = jnp.zeros((p_size, n_size), F32)
            for k in range(pairs + 1):
                acc += st_in[k, g, r * p_size:(r + 1) * p_size, :].astype(F32)
            top = acc.astype(BF16)
            state_ref[0, h] = top
            held = jnp.zeros((EDGE, p_size), F32)
            rest = acc
            for _ in range(3):
                term = rest.astype(BF16)
                held += lax.dot_general(query_rows, term, (((1,), (1,)), ((), ())), preferred_element_type=F32)
                rest = rest - term.astype(F32)
            helds.append(held[0:1])
        span = slice(g * gcols, (g + 1) * gcols)
        held_row = jnp.concatenate(helds, axis=1)
        inner_prod = jnp.sum(query * key, axis=1, keepdims=True)
        value_row = new_values[:, span]
        out = (decay_row[:, span] * held_row + (step_row[:, span] * inner_prod) * value_row
               + skip_row[:, span] * value_row)
        gated = out * silu(gate[:, span])
        ms = jnp.sum(gated * gated, axis=1, keepdims=True) / gcols
        normed = gated * lax.rsqrt(ms + EPS)
        for r in range(ratio):
            h = g * ratio + r
            read_s[h:h + 1, :] = normed[:, r * p_size:(r + 1) * p_size] * ng_ref[h:h + 1, :]
    read_ref[0] = read_s[...].astype(BF16)

    @pl.when(i == sp - 1)
    def _():
        for a in range(spt):
            for q in range(tp):
                either(a, q, tail(a, q)[0].wait_send, None)
    for k in range(sp):
        pl.when(i != k)(tot(k).wait_send)
    for s in range(steps):
        a_copy(s).wait_send()
        pl.when(far)(b_copy(s).wait_send)
        for gp in range(PAIR):
            here, remote, _ = state_copy(s, gp)
            pl.when(jnp.logical_not(far) & jnp.logical_not(here))(remote.wait_send)


def per_device(
    dims, x_in, x_new, w_x, w_b, w_c, w_dt, w_z, conv_w, conv_b, dt_bias, a_log, d_skip, norm_g
):
    sp, tp, heads, groups, n_size, p_size, ratio, taps = dims
    spt, length, width = x_in.shape
    hl, gl = heads // tp, groups // tp
    assert x_new.shape[0] == 1 and sp == spt * tp and spt == 2 and sp % 4 == 0
    steps, gcols = groups // PAIR, ratio * p_size
    tiles = PAIR * (gcols + n_size) // LANES
    any_spec = pl.BlockSpec(memory_space=pl.ANY)
    vmem = pl.BlockSpec(memory_space=pltpu.VMEM)
    dma = pltpu.SemaphoreType.DMA
    return pl.pallas_call(
        functools.partial(kernel, dims),
        out_shape=(
            jax.ShapeDtypeStruct((1, hl, p_size, n_size), BF16),
            jax.ShapeDtypeStruct((1, hl, p_size), BF16),
        ),
        in_specs=[any_spec, vmem] + [any_spec] * 7 + [vmem] * 4,
        out_specs=(vmem, vmem),
        scratch_shapes=[
            pltpu.VMEM((spt, EDGE + length, width), BF16),
            pltpu.VMEM((steps, width, PAIR * gcols), BF16),
            pltpu.VMEM((steps, width, PAIR * n_size), BF16),
            pltpu.VMEM((heads, width), BF16),
            pltpu.VMEM((width, hl * p_size), BF16),
            pltpu.VMEM((width, gl * n_size), BF16),
            pltpu.VMEM((width, gl * n_size), BF16),
            pltpu.VMEM((width, hl * p_size), BF16),
            pltpu.VMEM((2 * EDGE, width), BF16),
            pltpu.VMEM((tiles, EDGE + length, LANES), F32),
            pltpu.VMEM((tiles, EDGE + length, LANES), F32),
            pltpu.VMEM((length, LANES), F32),
            pltpu.VMEM((spt, heads, length), F32),
            pltpu.VMEM((8, LANES), F32),
            pltpu.VMEM((sp, 8, LANES), F32),
            pltpu.VMEM((steps, PAIR, gcols, n_size), BF16),
            pltpu.VMEM((steps, PAIR, gcols, n_size), BF16),
            pltpu.VMEM((steps, PAIR, gcols, n_size), BF16),
            pltpu.VMEM((steps, PAIR, gcols, n_size), BF16),
            pltpu.VMEM((steps, PAIR, gcols, n_size), BF16),
            pltpu.VMEM((sp // 4 + 1, gl, gcols, n_size), BF16),
            pltpu.VMEM((8, heads), F32),
            pltpu.VMEM((hl, p_size), F32),
            pltpu.VMEM(conv_w.shape, F32),
            pltpu.VMEM((1, conv_w.shape[1]), F32),
            dma((spt,)), dma, dma((steps, 2)), dma((4,)), dma((2,)), dma((spt,)), dma((spt,)),
            dma((spt, tp)), dma((1,)), dma((sp,)), dma((sp,)), dma((steps,)), dma((steps,)),
            dma((steps,)), dma((steps,)), dma((steps, PAIR)), dma((sp // 4 + 1, gl)),
        ],
        compiler_params=pltpu.CompilerParams(
            collective_id=0, has_side_effects=True, vmem_limit_bytes=60 * 1024 * 1024
        ),
    )(
        x_in, x_new, w_x, w_b, w_c, w_dt.T, w_z, conv_w, conv_b.reshape(1, -1),
        dt_bias.reshape(1, -1), a_log.reshape(1, -1), d_skip.reshape(1, -1), norm_g,
    )


def solution(mesh):
    sp, tp = mesh.shape["sp"], mesh.shape["tp"]

    def step(x_in, x_new, w_x, w_b, w_c, w_dt, w_z, conv_w, conv_b, dt_bias, a_log, d_skip, norm_g):
        heads, p_size = w_dt.shape[1], norm_g.shape[1]
        keys_all = w_b.shape[1]
        n_size = LANES
        groups = keys_all // n_size
        dims = (sp, tp, heads, groups, n_size, p_size, heads // groups, conv_w.shape[0])
        return per_device(
            dims, x_in, x_new, w_x, w_b, w_c, w_dt, w_z, conv_w, conv_b, dt_bias, a_log, d_skip, norm_g)

    return jax.shard_map(
        step,
        mesh=mesh,
        in_specs=(
            P("tp", "sp", None), P("sp", None), P(), P(), P(), P(), P(None, "tp"),
            P(), P(), P(), P(), P(), P("tp", None),
        ),
        out_specs=(P("sp", "tp", None, None), P("sp", "tp", None)),
        check_vma=False,
    )
```

```python
import functools

import jax
import jax.numpy as jnp
from jax import lax
from jax.experimental import pallas as pl
from jax.experimental.pallas import tpu as pltpu
from jax.sharding import PartitionSpec as P

MESH = pl.DeviceIdType.MESH
F32 = jnp.float32
BF16 = jnp.bfloat16
EPS = 1e-05
EDGE = 16
SENT = 8
PAIR = 2
LANES = 128


def silu(x):
    half = 0.5 * x
    return half + half * jnp.tanh(half)


def softplus(x):
    return jnp.maximum(x, 0.0) + jnp.log1p(jnp.exp(-jnp.abs(x)))


def rounded(x):
    return x.astype(BF16).astype(F32)


def kernel(
    dims,
    x_ref, xn_ref, wx_ref, wb_ref, wc_ref, wdt_ref, wz_ref,
    cw_hbm, cb_hbm, dtb_ref, alog_ref, dskip_ref, ng_ref,
    state_ref, read_ref,
    xs, wxs, wbs, wdts, wxn, wbn, wcn, wzn, nt, pre0, pre1, padded,
    wt, tot_out, tot_in, fcol, terms, a_out, a_in, mine, b_in, st_out, st_in, head_s, read_s, cw_ref, cb_ref,
    x_sem, wdt_sem, w_sem, new_sem, conv_sem, halo_send, halo_recv, tail_send, tail_recv, relay_send,
    tot_send, tot_recv, a_send, a_recv, b_send, b_recv, st_send, st_recv,
):
    sp, tp, heads, groups, n_size, p_size, ratio, taps = dims
    i, j = lax.axis_index("sp"), lax.axis_index("tp")
    spt, length, _ = x_ref.shape
    hl, gl = heads // tp, groups // tp
    inner, keys_all = heads * p_size, groups * n_size
    gcols = ratio * p_size
    steps = groups // PAIR
    home = i // spt
    pres = (pre0, pre1)
    member, m = lax.rem(i, 2), i // 2
    direct = m // 2 == j // 2
    near = jnp.logical_not(direct) & ((j > m) == (lax.rem(m, 2) == 1))
    far = jnp.logical_not(direct) & jnp.logical_not(near)
    partner, sibling = i + 1 - 2 * member, i + 2 - 4 * lax.rem(m, 2)
    pairs = sp // 4

    nt[0:EDGE - SENT, :] = jnp.zeros((EDGE - SENT, nt.shape[1]), BF16)
    for a in range(spt):
        xs[a, 0:EDGE - SENT, :] = jnp.zeros((EDGE - SENT, nt.shape[1]), BF16)

    barrier = pltpu.get_barrier_semaphore()
    for k in range(sp):
        @pl.when(i != k)
        def _():
            pl.semaphore_signal(barrier, inc=1, device_id={"sp": k, "tp": j}, device_id_type=MESH)

        @pl.when(home != j)
        def _():
            pl.semaphore_signal(barrier, inc=1, device_id={"sp": k, "tp": home}, device_id_type=MESH)
    after = lax.rem(i + 1, sp)

    wdt_copy = pltpu.make_async_copy(wdt_ref, wdts, wdt_sem)
    x_copies = [
        pltpu.make_async_copy(x_ref.at[a], xs.at[a, pl.ds(EDGE, length)], x_sem.at[a])
        for a in range(spt)
    ]
    w_copies = []
    for s in range(steps):
        w_copies.append((
            pltpu.make_async_copy(
                wx_ref.at[:, pl.ds(s * PAIR * gcols, PAIR * gcols)], wxs.at[s], w_sem.at[s, 0]),
            pltpu.make_async_copy(
                wb_ref.at[:, pl.ds(s * PAIR * n_size, PAIR * n_size)], wbs.at[s], w_sem.at[s, 1]),
        ))
    vcol = pl.multiple_of(j * (hl * p_size), LANES)
    gcol = pl.multiple_of(j * (gl * n_size), LANES)
    new_copies = [
        pltpu.make_async_copy(wx_ref.at[:, pl.ds(vcol, hl * p_size)], wxn, new_sem.at[0]),
        pltpu.make_async_copy(wb_ref.at[:, pl.ds(gcol, gl * n_size)], wbn, new_sem.at[1]),
        pltpu.make_async_copy(wc_ref.at[:, pl.ds(gcol, gl * n_size)], wcn, new_sem.at[2]),
        pltpu.make_async_copy(wz_ref, wzn, new_sem.at[3]),
    ]
    conv_copies = [
        pltpu.make_async_copy(cw_hbm, cw_ref, conv_sem.at[0]),
        pltpu.make_async_copy(cb_hbm, cb_ref, conv_sem.at[1]),
    ]
    wdt_copy.start()
    for c in x_copies:
        c.start()
    for pair in w_copies[:1]:
        for c in pair:
            c.start()
    for c in conv_copies:
        c.start()
    for pair in w_copies[1:]:
        for c in pair:
            c.start()
    for c in new_copies:
        c.start()

    pl.semaphore_wait(barrier, sp - 1 + spt * (tp - 1))

    def halo(a):
        return pltpu.make_async_remote_copy(
            src_ref=x_ref.at[a, pl.ds(length - SENT, SENT)],
            dst_ref=xs.at[a, pl.ds(EDGE - SENT, SENT)],
            send_sem=halo_send.at[a], recv_sem=halo_recv.at[a],
            device_id={"sp": after, "tp": j}, device_id_type=MESH)

    for a in range(spt):
        halo(a).start()

    root = home == j

    def tail(a):
        src, dst = x_ref.at[a, pl.ds(length - SENT, SENT)], nt.at[pl.ds(EDGE - SENT, SENT)]
        return spt * j + a == i, pltpu.make_async_remote_copy(
            src_ref=src, dst_ref=dst, send_sem=tail_send.at[a], recv_sem=tail_recv.at[0],
            device_id={"sp": spt * j + a, "tp": j}, device_id_type=MESH
        ), pltpu.make_async_copy(src, dst, tail_recv.at[0])

    def relay(q):
        rows = nt.at[pl.ds(EDGE - SENT, SENT)]
        return pltpu.make_async_remote_copy(
            src_ref=rows, dst_ref=rows, send_sem=relay_send.at[q], recv_sem=tail_recv.at[0],
            device_id={"sp": i, "tp": q}, device_id_type=MESH)

    @pl.when(i == sp - 1)
    def _():
        for a in range(spt):
            here, remote, local = tail(a)
            pl.when(jnp.logical_not(here))(remote.start)
            pl.when(here)(local.start)

    padded[...] = jnp.zeros_like(padded)

    def column(row):
        padded[0:1, 0:heads] = row
        return jnp.broadcast_to(padded[0:1, :], (LANES, LANES)).T[0:heads]

    rate_row = -jnp.exp(alog_ref[...])
    rates = column(rate_row)

    rows = lax.broadcasted_iota(jnp.int32, (length, length), 0)
    cols = lax.broadcasted_iota(jnp.int32, (length, length), 1)
    later = (rows > cols).astype(F32).astype(BF16)
    wdt_copy.wait()

    def tot(k):
        return pltpu.make_async_remote_copy(
            src_ref=tot_out, dst_ref=tot_in.at[i], send_sem=tot_send.at[k], recv_sem=tot_recv.at[i],
            device_id={"sp": k, "tp": j}, device_id_type=MESH)

    tot_out[...] = jnp.zeros_like(tot_out)
    for a in range(spt):
        x_copies[a].wait()
        raw = lax.dot_general(
            xs[a, EDGE:, :], wdts[...], (((1,), (1,)), ((), ())), preferred_element_type=F32)
        padded[:, 0:heads] = softplus(rounded(raw) + dtb_ref[...])
        tot_out[a:a + 1, :] = jnp.sum(padded[...], axis=0, keepdims=True)
        sizes = padded[...].T[0:heads]
        rest = jnp.zeros_like(sizes)
        left = sizes
        for _ in range(3):
            term = left.astype(BF16)
            rest += jnp.dot(term, later, preferred_element_type=F32)
            left = left - term.astype(F32)
        wt[a] = jnp.exp(rates[:, 0:1] * rest) * sizes
    tot_in[i] = tot_out[...]
    for k in range(sp):
        pl.when(i != k)(tot(k).start)

    for a in range(spt):
        halo(a).wait()
        xs[a, 0:EDGE, :] = jnp.where(i == 0, 0.0, xs[a, 0:EDGE, :].astype(F32)).astype(BF16)

    def later_factors():
        for k in range(sp):
            @pl.when(i != k)
            def _():
                pltpu.make_async_remote_copy(
                    src_ref=tot_out, dst_ref=tot_in.at[k], send_sem=tot_send.at[k], recv_sem=tot_recv.at[k],
                    device_id={"sp": k, "tp": j}, device_id_type=MESH).wait_recv()
        beyond = jnp.zeros(tot_out.shape, F32)
        for k in range(sp):
            beyond = beyond + jnp.where(k > i, tot_in[k], 0.0)
        for a in range(spt):
            fcol[a] = column(jnp.exp(rate_row * beyond[a:a + 1, 0:heads]))

    def a_copy(s):
        return pltpu.make_async_remote_copy(
            src_ref=a_out.at[s], dst_ref=a_in.at[s], send_sem=a_send.at[s], recv_sem=a_recv.at[s],
            device_id={"sp": partner, "tp": j}, device_id_type=MESH)

    def b_copy(s):
        return pltpu.make_async_remote_copy(
            src_ref=st_out.at[s], dst_ref=b_in.at[s], send_sem=b_send.at[s], recv_sem=b_recv.at[s],
            device_id={"sp": sibling, "tp": j}, device_id_type=MESH)

    slot = jnp.where(direct & (lax.rem(m, 2) == 1), pairs, m // 2)

    def state_copy(s, gp):
        g = s * PAIR + gp
        q = g // gl
        src, dst = st_out.at[s, gp], st_in.at[slot, lax.rem(g, gl)]
        sem = st_recv.at[slot, lax.rem(g, gl)]
        return (m == j) & (q == j), pltpu.make_async_remote_copy(
            src_ref=src, dst_ref=dst, send_sem=st_send.at[s, gp], recv_sem=sem,
            device_id={"sp": spt * j + member, "tp": q}, device_id_type=MESH
        ), pltpu.make_async_copy(src, dst, sem)

    def pass_on(s):
        a_copy(s).wait_recv()

        def add(*more):
            for gp in range(PAIR):
                for r in range(0, gcols, LANES):
                    total = mine[s, gp, r:r + LANES, :].astype(F32)
                    for ref in more:
                        total += ref[s, gp, r:r + LANES, :].astype(F32)
                    st_out[s, gp, r:r + LANES, :] = total.astype(BF16)

        @pl.when(near)
        def _():
            b_copy(s).wait_recv()
            add(a_in, b_in)

        @pl.when(jnp.logical_not(near))
        def _():
            add(a_in)

        @pl.when(far)
        def _():
            b_copy(s).start()

        @pl.when(jnp.logical_not(far))
        def _():
            for gp in range(PAIR):
                here, remote, local = state_copy(s, gp)
                pl.when(jnp.logical_not(here))(remote.start)
                pl.when(here)(local.start)

    lag = jnp.where(near, 2, 1)
    for c in conv_copies:
        c.wait()

    vtiles, ktiles = PAIR * gcols // LANES, PAIR * n_size // LANES
    tiles_group = gcols // LANES
    heads_tile = LANES // p_size

    def step(s, carry):
        pltpu.make_async_copy(wx_ref.at[:, pl.ds(0, PAIR * gcols)], wxs.at[s], w_sem.at[s, 0]).wait()
        pltpu.make_async_copy(wb_ref.at[:, pl.ds(0, PAIR * n_size)], wbs.at[s], w_sem.at[s, 1]).wait()

        def project(a):
            values = jnp.dot(xs[a], wxs[s], preferred_element_type=F32)
            for c in range(vtiles):
                pres[a % 2][c] = rounded(values[:, c * LANES:(c + 1) * LANES])
            keys = jnp.dot(xs[a], wbs[s], preferred_element_type=F32)
            for c in range(ktiles):
                pres[a % 2][vtiles + c] = rounded(keys[:, c * LANES:(c + 1) * LANES])

        def conv(a, c):
            if c < vtiles:
                at = pl.multiple_of(s * (PAIR * gcols) + c * LANES, LANES)
            else:
                at = pl.multiple_of(inner + s * (PAIR * n_size) + (c - vtiles) * LANES, LANES)
            acc = cb_ref[:, pl.ds(at, LANES)]
            w = cw_ref[:, pl.ds(at, LANES)]
            for o in range(taps):
                acc = acc + w[o:o + 1] * pres[a % 2][c, pl.ds(EDGE - taps + 1 + o, length), :]
            return silu(acc).astype(BF16)

        def contract(a):
            weights = wt[a, pl.ds(pl.multiple_of(s * (PAIR * ratio), PAIR * ratio), PAIR * ratio), :]
            for gp in range(PAIR):
                key = conv(a, vtiles + gp)
                parts = []
                for c in range(gp * tiles_group, (gp + 1) * tiles_group):
                    turned = conv(a, c).T
                    for r in range(heads_tile):
                        h = c * heads_tile + r
                        part = turned[r * p_size:(r + 1) * p_size].astype(F32)
                        parts.append((weights[h:h + 1] * part).astype(BF16))
                scaled = jnp.concatenate(parts, axis=0)
                terms[a, gp] = jnp.dot(scaled, key, preferred_element_type=F32)

        for a in range(spt):
            project(a)
            if a > 0:
                contract(a - 1)
        contract(spt - 1)
        pl.when(s == 0)(later_factors)
        at = pl.multiple_of(s * (PAIR * ratio), PAIR * ratio)
        factors = [fcol[a, pl.ds(at, PAIR * ratio), :] for a in range(spt)]
        for gp in range(PAIR):
            for r in range(ratio):
                h, span = gp * ratio + r, slice(r * p_size, (r + 1) * p_size)
                first, second = (factors[a][h:h + 1] * terms[a, gp, span, :] for a in range(spt))
                a_out[s, gp, span, :] = jnp.where(member == 0, second, first).astype(BF16)
                mine[s, gp, span, :] = jnp.where(member == 0, first, second).astype(BF16)
        a_copy(s).start()
        pl.when(s >= lag)(lambda: pass_on(s - lag))

        @pl.when(root & (s == steps - 1))
        def _():
            tail(0)[1].wait_recv()
            for q in range(tp):
                pl.when(q != j)(relay(q).start)

        return carry

    lax.fori_loop(0, steps, step, 0)

    newest = jnp.broadcast_to(xn_ref[...].astype(F32), (EDGE, xn_ref.shape[1])).astype(BF16)
    nt[EDGE:2 * EDGE, :] = newest
    pl.when(jnp.logical_not(root))(tail(0)[1].wait_recv)
    for c in new_copies:
        c.wait()

    def new_conv(w_ref, start, width):
        pre = rounded(jnp.dot(nt[...], w_ref[...], preferred_element_type=F32))
        start = pl.multiple_of(start, LANES)
        acc = cb_ref[:, pl.ds(start, width)]
        w = cw_ref[:, pl.ds(start, width)]
        for o in range(taps):
            at = EDGE - taps + 1 + o
            acc = acc + w[o:o + 1] * pre[at:at + 1]
        return rounded(silu(acc))

    new_values = new_conv(wxn, vcol, hl * p_size)
    new_keys = new_conv(wbn, inner + gcol, gl * n_size)
    new_query = new_conv(wcn, inner + keys_all + gcol, gl * n_size)
    gate = rounded(jnp.dot(newest, wzn[...], preferred_element_type=F32)[0:1])
    new_raw = rounded(lax.dot_general(
        newest, wdts[...], (((1,), (1,)), ((), ())), preferred_element_type=F32)[0:1])
    new_steps = softplus(new_raw + dtb_ref[...])
    head_s[...] = jnp.zeros_like(head_s)
    head_s[0:1, :] = new_steps
    head_s[1:2, :] = jnp.exp(-jnp.exp(alog_ref[...]) * new_steps)
    head_s[2:3, :] = dskip_ref[...]
    hrow = lax.broadcasted_iota(jnp.int32, (heads, hl * p_size), 0)
    hcol = lax.broadcasted_iota(jnp.int32, (heads, hl * p_size), 1)
    first = j * hl
    onehot = ((hcol >= (hrow - first) * p_size) & (hcol < (hrow - first + 1) * p_size)).astype(F32)
    spread_rows = jnp.dot(head_s[...], onehot, precision=lax.Precision.HIGHEST, preferred_element_type=F32)
    step_row, decay_row, skip_row = spread_rows[0:1], spread_rows[1:2], spread_rows[2:3]

    pass_on(steps - lag)
    pl.when(near)(lambda: pass_on(steps - 1))
    for g in range(gl):
        for k in range(pairs + 1):
            pltpu.make_async_remote_copy(
                src_ref=st_out.at[0, 0], dst_ref=st_in.at[k, g], send_sem=st_send.at[0, 0],
                recv_sem=st_recv.at[k, g], device_id={"sp": after, "tp": j}, device_id_type=MESH).wait_recv()
        query = new_query[:, g * n_size:(g + 1) * n_size]
        key = new_keys[:, g * n_size:(g + 1) * n_size]
        query_rows = jnp.broadcast_to(query, (EDGE, n_size)).astype(BF16)
        helds = []
        for r in range(ratio):
            h = g * ratio + r
            acc = jnp.zeros((p_size, n_size), F32)
            for k in range(pairs + 1):
                acc += st_in[k, g, r * p_size:(r + 1) * p_size, :].astype(F32)
            top = acc.astype(BF16)
            state_ref[0, h] = top
            held = jnp.zeros((EDGE, p_size), F32)
            rest = acc
            for _ in range(3):
                term = rest.astype(BF16)
                held += lax.dot_general(query_rows, term, (((1,), (1,)), ((), ())), preferred_element_type=F32)
                rest = rest - term.astype(F32)
            helds.append(held[0:1])
        span = slice(g * gcols, (g + 1) * gcols)
        held_row = jnp.concatenate(helds, axis=1)
        inner_prod = jnp.sum(query * key, axis=1, keepdims=True)
        value_row = new_values[:, span]
        out = (decay_row[:, span] * held_row + (step_row[:, span] * inner_prod) * value_row
               + skip_row[:, span] * value_row)
        gated = out * silu(gate[:, span])
        ms = jnp.sum(gated * gated, axis=1, keepdims=True) / gcols
        normed = gated * lax.rsqrt(ms + EPS)
        for r in range(ratio):
            h = g * ratio + r
            read_s[h:h + 1, :] = normed[:, r * p_size:(r + 1) * p_size] * ng_ref[h:h + 1, :]
    read_ref[0] = read_s[...].astype(BF16)

    @pl.when(i == sp - 1)
    def _():
        for a in range(spt):
            here, remote, _ = tail(a)
            pl.when(jnp.logical_not(here))(remote.wait_send)

    for q in range(tp):
        pl.when(root & (q != j))(relay(q).wait_send)
    for k in range(sp):
        pl.when(i != k)(tot(k).wait_send)
    for s in range(steps):
        a_copy(s).wait_send()
        pl.when(far)(b_copy(s).wait_send)
        for gp in range(PAIR):
            here, remote, _ = state_copy(s, gp)
            pl.when(jnp.logical_not(far) & jnp.logical_not(here))(remote.wait_send)


def per_device(
    dims, x_in, x_new, w_x, w_b, w_c, w_dt, w_z, conv_w, conv_b, dt_bias, a_log, d_skip, norm_g
):
    sp, tp, heads, groups, n_size, p_size, ratio, taps = dims
    spt, length, width = x_in.shape
    hl, gl = heads // tp, groups // tp
    assert x_new.shape[0] == 1 and sp == spt * tp and spt == 2 and sp % 4 == 0
    steps, gcols = groups // PAIR, ratio * p_size
    tiles = PAIR * (gcols + n_size) // LANES
    any_spec = pl.BlockSpec(memory_space=pl.ANY)
    vmem = pl.BlockSpec(memory_space=pltpu.VMEM)
    dma = pltpu.SemaphoreType.DMA
    return pl.pallas_call(
        functools.partial(kernel, dims),
        out_shape=(
            jax.ShapeDtypeStruct((1, hl, p_size, n_size), BF16),
            jax.ShapeDtypeStruct((1, hl, p_size), BF16),
        ),
        in_specs=[any_spec, vmem] + [any_spec] * 7 + [vmem] * 4,
        out_specs=(vmem, vmem),
        scratch_shapes=[
            pltpu.VMEM((spt, EDGE + length, width), BF16),
            pltpu.VMEM((steps, width, PAIR * gcols), BF16),
            pltpu.VMEM((steps, width, PAIR * n_size), BF16),
            pltpu.VMEM((heads, width), BF16),
            pltpu.VMEM((width, hl * p_size), BF16),
            pltpu.VMEM((width, gl * n_size), BF16),
            pltpu.VMEM((width, gl * n_size), BF16),
            pltpu.VMEM((width, hl * p_size), BF16),
            pltpu.VMEM((2 * EDGE, width), BF16),
            pltpu.VMEM((tiles, EDGE + length, LANES), F32),
            pltpu.VMEM((tiles, EDGE + length, LANES), F32),
            pltpu.VMEM((length, LANES), F32),
            pltpu.VMEM((spt, heads, length), F32),
            pltpu.VMEM((8, LANES), F32),
            pltpu.VMEM((sp, 8, LANES), F32),
            pltpu.VMEM((spt, heads, LANES), F32),
            pltpu.VMEM((spt, PAIR, gcols, n_size), F32),
            pltpu.VMEM((steps, PAIR, gcols, n_size), BF16),
            pltpu.VMEM((steps, PAIR, gcols, n_size), BF16),
            pltpu.VMEM((steps, PAIR, gcols, n_size), BF16),
            pltpu.VMEM((steps, PAIR, gcols, n_size), BF16),
            pltpu.VMEM((steps, PAIR, gcols, n_size), BF16),
            pltpu.VMEM((sp // 4 + 1, gl, gcols, n_size), BF16),
            pltpu.VMEM((8, heads), F32),
            pltpu.VMEM((hl, p_size), F32),
            pltpu.VMEM(conv_w.shape, F32),
            pltpu.VMEM((1, conv_w.shape[1]), F32),
            dma((spt,)), dma, dma((steps, 2)), dma((4,)), dma((2,)), dma((spt,)), dma((spt,)),
            dma((spt,)), dma((1,)), dma((tp,)), dma((sp,)), dma((sp,)), dma((steps,)), dma((steps,)),
            dma((steps,)), dma((steps,)), dma((steps, PAIR)), dma((sp // 4 + 1, gl)),
        ],
        compiler_params=pltpu.CompilerParams(
            collective_id=0, has_side_effects=True, vmem_limit_bytes=60 * 1024 * 1024
        ),
    )(
        x_in, x_new, w_x, w_b, w_c, w_dt.T, w_z, conv_w, conv_b.reshape(1, -1),
        dt_bias.reshape(1, -1), a_log.reshape(1, -1), d_skip.reshape(1, -1), norm_g,
    )


def solution(mesh):
    sp, tp = mesh.shape["sp"], mesh.shape["tp"]

    def step(x_in, x_new, w_x, w_b, w_c, w_dt, w_z, conv_w, conv_b, dt_bias, a_log, d_skip, norm_g):
        heads, p_size = w_dt.shape[1], norm_g.shape[1]
        keys_all = w_b.shape[1]
        n_size = LANES
        groups = keys_all // n_size
        dims = (sp, tp, heads, groups, n_size, p_size, heads // groups, conv_w.shape[0])
        return per_device(
            dims, x_in, x_new, w_x, w_b, w_c, w_dt, w_z, conv_w, conv_b, dt_bias, a_log, d_skip, norm_g)

    return jax.shard_map(
        step,
        mesh=mesh,
        in_specs=(
            P("tp", "sp", None), P("sp", None), P(), P(), P(), P(), P(None, "tp"),
            P(), P(), P(), P(), P(), P("tp", None),
        ),
        out_specs=(P("sp", "tp", None, None), P("sp", "tp", None)),
        check_vma=False,
    )
```

```python
import functools

import jax
import jax.numpy as jnp
from jax import lax
from jax.experimental import pallas as pl
from jax.experimental.pallas import tpu as pltpu
from jax.sharding import PartitionSpec as P

MESH = pl.DeviceIdType.MESH
F32 = jnp.float32
BF16 = jnp.bfloat16
EPS = 1e-05
EDGE = 16
SENT = 8
PAIR = 2
LANES = 128


def silu(x):
    half = 0.5 * x
    return half + half * jnp.tanh(half)


def softplus(x):
    return jnp.maximum(x, 0.0) + jnp.log1p(jnp.exp(-jnp.abs(x)))


def rounded(x):
    return x.astype(BF16).astype(F32)


def kernel(
    dims,
    x_ref, xn_ref, wx_ref, wb_ref, wc_ref, wdt_ref, wz_ref,
    cw_hbm, cb_hbm, dtb_ref, alog_ref, dskip_ref, ng_ref,
    state_ref, read_ref,
    xs, wxs, wbs, wdts, wn, pre_n, nt, pre0, pre1, padded,
    wt, tot_out, tot_in, fcol, terms, a_out, a_in, mine, b_in, st_out, st_in, head_s, read_s, cw_ref, cb_ref,
    x_sem, wdt_sem, w_sem, new_sem, conv_sem, halo_send, halo_recv, tail_send, tail_recv, relay_send,
    tot_send, tot_recv, a_send, a_recv, b_send, b_recv, st_send, st_recv,
):
    sp, tp, heads, groups, n_size, p_size, ratio, taps = dims
    i, j = lax.axis_index("sp"), lax.axis_index("tp")
    spt, length, _ = x_ref.shape
    hl, gl = heads // tp, groups // tp
    inner, keys_all = heads * p_size, groups * n_size
    gcols = ratio * p_size
    steps = groups // PAIR
    home = i // spt
    pres = (pre0, pre1)
    member, m = lax.rem(i, 2), i // 2
    direct = m // 2 == j // 2
    near = jnp.logical_not(direct) & ((j > m) == (lax.rem(m, 2) == 1))
    far = jnp.logical_not(direct) & jnp.logical_not(near)
    partner, sibling = i + 1 - 2 * member, i + 2 - 4 * lax.rem(m, 2)
    pairs = sp // 4

    nt[0:EDGE - SENT, :] = jnp.zeros((EDGE - SENT, nt.shape[1]), BF16)
    for a in range(spt):
        xs[a, 0:EDGE - SENT, :] = jnp.zeros((EDGE - SENT, nt.shape[1]), BF16)

    barrier = pltpu.get_barrier_semaphore()
    for k in range(sp):
        @pl.when(i != k)
        def _():
            pl.semaphore_signal(barrier, inc=1, device_id={"sp": k, "tp": j}, device_id_type=MESH)

        @pl.when(home != j)
        def _():
            pl.semaphore_signal(barrier, inc=1, device_id={"sp": k, "tp": home}, device_id_type=MESH)
    after = lax.rem(i + 1, sp)

    wdt_copy = pltpu.make_async_copy(wdt_ref, wdts, wdt_sem)
    x_copies = [
        pltpu.make_async_copy(x_ref.at[a], xs.at[a, pl.ds(EDGE, length)], x_sem.at[a])
        for a in range(spt)
    ]
    w_copies = []
    for s in range(steps):
        w_copies.append((
            pltpu.make_async_copy(
                wx_ref.at[:, pl.ds(s * PAIR * gcols, PAIR * gcols)], wxs.at[s], w_sem.at[s, 0]),
            pltpu.make_async_copy(
                wb_ref.at[:, pl.ds(s * PAIR * n_size, PAIR * n_size)], wbs.at[s], w_sem.at[s, 1]),
        ))
    vcol = pl.multiple_of(j * (hl * p_size), LANES)
    gcol = pl.multiple_of(j * (gl * n_size), LANES)
    part = gl * n_size
    vparts = hl * p_size // part
    sources = [wx_ref.at[:, pl.ds(pl.multiple_of(vcol + c * part, LANES), part)] for c in range(vparts)]
    sources += [wb_ref.at[:, pl.ds(gcol, part)], wc_ref.at[:, pl.ds(gcol, part)]]
    sources += [wz_ref.at[:, pl.ds(c * part, part)] for c in range(vparts)]
    new_copies = [
        pltpu.make_async_copy(src, wn.at[c], new_sem.at[c]) for c, src in enumerate(sources)
    ]
    conv_copies = [
        pltpu.make_async_copy(cw_hbm, cw_ref, conv_sem.at[0]),
        pltpu.make_async_copy(cb_hbm, cb_ref, conv_sem.at[1]),
    ]
    wdt_copy.start()
    for c in x_copies:
        c.start()
    for pair in w_copies[:1]:
        for c in pair:
            c.start()
    for c in conv_copies:
        c.start()
    for pair in w_copies[1:]:
        for c in pair:
            c.start()
    for c in new_copies:
        c.start()

    pl.semaphore_wait(barrier, sp - 1 + spt * (tp - 1))

    def halo(a):
        return pltpu.make_async_remote_copy(
            src_ref=x_ref.at[a, pl.ds(length - SENT, SENT)],
            dst_ref=xs.at[a, pl.ds(EDGE - SENT, SENT)],
            send_sem=halo_send.at[a], recv_sem=halo_recv.at[a],
            device_id={"sp": after, "tp": j}, device_id_type=MESH)

    for a in range(spt):
        halo(a).start()

    root = home == j

    def tail(a):
        src, dst = x_ref.at[a, pl.ds(length - SENT, SENT)], nt.at[pl.ds(EDGE - SENT, SENT)]
        return spt * j + a == i, pltpu.make_async_remote_copy(
            src_ref=src, dst_ref=dst, send_sem=tail_send.at[a], recv_sem=tail_recv.at[0],
            device_id={"sp": spt * j + a, "tp": j}, device_id_type=MESH
        ), pltpu.make_async_copy(src, dst, tail_recv.at[0])

    def relay(q):
        rows = nt.at[pl.ds(EDGE - SENT, SENT)]
        return pltpu.make_async_remote_copy(
            src_ref=rows, dst_ref=rows, send_sem=relay_send.at[q], recv_sem=tail_recv.at[0],
            device_id={"sp": i, "tp": q}, device_id_type=MESH)

    @pl.when(i == sp - 1)
    def _():
        for a in range(spt):
            here, remote, local = tail(a)
            pl.when(jnp.logical_not(here))(remote.start)
            pl.when(here)(local.start)

    padded[...] = jnp.zeros_like(padded)

    def column(row):
        padded[0:1, 0:heads] = row
        return jnp.broadcast_to(padded[0:1, :], (LANES, LANES)).T[0:heads]

    rate_row = -jnp.exp(alog_ref[...])
    rates = column(rate_row)

    rows = lax.broadcasted_iota(jnp.int32, (length, length), 0)
    cols = lax.broadcasted_iota(jnp.int32, (length, length), 1)
    later = (rows > cols).astype(F32).astype(BF16)
    wdt_copy.wait()

    def tot(k):
        return pltpu.make_async_remote_copy(
            src_ref=tot_out, dst_ref=tot_in.at[i], send_sem=tot_send.at[k], recv_sem=tot_recv.at[i],
            device_id={"sp": k, "tp": j}, device_id_type=MESH)

    tot_out[...] = jnp.zeros_like(tot_out)
    def sizes_of(a, carry):
        pltpu.make_async_copy(x_ref.at[a], xs.at[a, pl.ds(EDGE, length)], x_sem.at[a]).wait()
        raw = lax.dot_general(
            xs[a, EDGE:, :], wdts[...], (((1,), (1,)), ((), ())), preferred_element_type=F32)
        padded[:, 0:heads] = softplus(rounded(raw) + dtb_ref[...])
        tot_out[pl.ds(a, 1), :] = jnp.sum(padded[...], axis=0, keepdims=True)
        sizes = padded[...].T[0:heads]
        split, left = [], sizes
        for _ in range(3):
            split.append(left.astype(BF16))
            left = left - split[-1].astype(F32)
        parts = jnp.dot(jnp.concatenate(split, axis=0), later, preferred_element_type=F32)
        rest = parts[0:heads] + parts[heads:2 * heads] + parts[2 * heads:3 * heads]
        wt[a] = jnp.exp(rates[:, 0:1] * rest) * sizes
        return carry

    lax.fori_loop(0, spt, sizes_of, 0)
    tot_in[i] = tot_out[...]
    for k in range(sp):
        pl.when(i != k)(tot(k).start)

    for a in range(spt):
        halo(a).wait()
        xs[a, 0:EDGE, :] = jnp.where(i == 0, 0.0, xs[a, 0:EDGE, :].astype(F32)).astype(BF16)

    def later_factors():
        for k in range(sp):
            @pl.when(i != k)
            def _():
                pltpu.make_async_remote_copy(
                    src_ref=tot_out, dst_ref=tot_in.at[k], send_sem=tot_send.at[k], recv_sem=tot_recv.at[k],
                    device_id={"sp": k, "tp": j}, device_id_type=MESH).wait_recv()
        beyond = jnp.zeros(tot_out.shape, F32)
        for k in range(sp):
            beyond = beyond + jnp.where(k > i, tot_in[k], 0.0)
        for a in range(spt):
            fcol[a] = column(jnp.exp(rate_row * beyond[a:a + 1, 0:heads]))

    def a_copy(s, gp):
        return pltpu.make_async_remote_copy(
            src_ref=a_out.at[s, gp], dst_ref=a_in.at[s, gp],
            send_sem=a_send.at[s, gp], recv_sem=a_recv.at[s, gp],
            device_id={"sp": partner, "tp": j}, device_id_type=MESH)

    def b_copy(s, gp):
        return pltpu.make_async_remote_copy(
            src_ref=st_out.at[s, gp], dst_ref=b_in.at[s, gp],
            send_sem=b_send.at[s, gp], recv_sem=b_recv.at[s, gp],
            device_id={"sp": sibling, "tp": j}, device_id_type=MESH)

    slot = jnp.where(direct & (lax.rem(m, 2) == 1), pairs, m // 2)

    def state_copy(s, gp):
        g = s * PAIR + gp
        q = g // gl
        src, dst = st_out.at[s, gp], st_in.at[slot, lax.rem(g, gl)]
        sem = st_recv.at[slot, lax.rem(g, gl)]
        return (m == j) & (q == j), pltpu.make_async_remote_copy(
            src_ref=src, dst_ref=dst, send_sem=st_send.at[s, gp], recv_sem=sem,
            device_id={"sp": spt * j + member, "tp": q}, device_id_type=MESH
        ), pltpu.make_async_copy(src, dst, sem)

    def pass_on(s):
        def piece(gp, carry):
            a_copy(s, gp).wait_recv()

            def add(*more):
                for r in range(0, gcols, LANES):
                    total = mine[s, gp, r:r + LANES, :].astype(F32)
                    for ref in more:
                        total += ref[s, gp, r:r + LANES, :].astype(F32)
                    st_out[s, gp, r:r + LANES, :] = total.astype(BF16)

            @pl.when(near)
            def _():
                b_copy(s, gp).wait_recv()
                add(a_in, b_in)

            @pl.when(jnp.logical_not(near))
            def _():
                add(a_in)

            pl.when(far)(b_copy(s, gp).start)

            @pl.when(jnp.logical_not(far))
            def _():
                here, remote, local = state_copy(s, gp)
                pl.when(jnp.logical_not(here))(remote.start)
                pl.when(here)(local.start)

            return carry

        lax.fori_loop(0, PAIR, piece, 0)

    lag = jnp.where(near, 2, 1)
    for c in conv_copies:
        c.wait()

    vtiles, ktiles = PAIR * gcols // LANES, PAIR * n_size // LANES
    tiles_group = gcols // LANES
    heads_tile = LANES // p_size

    def step(s, carry):
        pltpu.make_async_copy(wx_ref.at[:, pl.ds(0, PAIR * gcols)], wxs.at[s], w_sem.at[s, 0]).wait()
        pltpu.make_async_copy(wb_ref.at[:, pl.ds(0, PAIR * n_size)], wbs.at[s], w_sem.at[s, 1]).wait()

        def project(a):
            values = jnp.dot(xs[a], wxs[s], preferred_element_type=F32)
            for c in range(vtiles):
                pres[a % 2][c] = rounded(values[:, c * LANES:(c + 1) * LANES])
            keys = jnp.dot(xs[a], wbs[s], preferred_element_type=F32)
            for c in range(ktiles):
                pres[a % 2][vtiles + c] = rounded(keys[:, c * LANES:(c + 1) * LANES])

        def conv(a, c):
            if c < vtiles:
                at = pl.multiple_of(s * (PAIR * gcols) + c * LANES, LANES)
            else:
                at = pl.multiple_of(inner + s * (PAIR * n_size) + (c - vtiles) * LANES, LANES)
            acc = cb_ref[:, pl.ds(at, LANES)]
            w = cw_ref[:, pl.ds(at, LANES)]
            for o in range(taps):
                acc = acc + w[o:o + 1] * pres[a % 2][c, pl.ds(EDGE - taps + 1 + o, length), :]
            return silu(acc).astype(BF16)

        def contract(a):
            weights = wt[a, pl.ds(pl.multiple_of(s * (PAIR * ratio), PAIR * ratio), PAIR * ratio), :]
            for gp in range(PAIR):
                key = conv(a, vtiles + gp)
                parts = []
                for c in range(gp * tiles_group, (gp + 1) * tiles_group):
                    turned = conv(a, c).T
                    for r in range(heads_tile):
                        h = c * heads_tile + r
                        part = turned[r * p_size:(r + 1) * p_size].astype(F32)
                        parts.append((weights[h:h + 1] * part).astype(BF16))
                scaled = jnp.concatenate(parts, axis=0)
                terms[a, gp] = jnp.dot(scaled, key, preferred_element_type=F32)

        for a in range(spt):
            project(a)
            if a > 0:
                contract(a - 1)
        contract(spt - 1)
        pl.when(s == 0)(later_factors)
        at = pl.multiple_of(s * (PAIR * ratio), PAIR * ratio)
        factors = [fcol[a, pl.ds(at, PAIR * ratio), :] for a in range(spt)]
        for gp in range(PAIR):
            for r in range(ratio):
                h, span = gp * ratio + r, slice(r * p_size, (r + 1) * p_size)
                first, second = (factors[a][h:h + 1] * terms[a, gp, span, :] for a in range(spt))
                a_out[s, gp, span, :] = jnp.where(member == 0, second, first).astype(BF16)
                mine[s, gp, span, :] = jnp.where(member == 0, first, second).astype(BF16)
            a_copy(s, gp).start()
        pl.when(s >= lag)(lambda: pass_on(s - lag))

        @pl.when(root & (s == steps - 1))
        def _():
            tail(0)[1].wait_recv()
            for q in range(tp):
                pl.when(q != j)(relay(q).start)

        return carry

    lax.fori_loop(0, steps, step, 0)

    newest = jnp.broadcast_to(xn_ref[...].astype(F32), (EDGE, xn_ref.shape[1])).astype(BF16)
    nt[EDGE:2 * EDGE, :] = newest
    pl.when(jnp.logical_not(root))(tail(0)[1].wait_recv)
    for c in new_copies:
        c.wait()

    def new_rows(c, carry):
        pre_n[c] = rounded(jnp.dot(nt[...], wn[c], preferred_element_type=F32))
        return carry

    lax.fori_loop(0, len(sources), new_rows, 0)

    def new_conv(c, start):
        start = pl.multiple_of(start, LANES)
        acc = cb_ref[:, pl.ds(start, part)]
        w = cw_ref[:, pl.ds(start, part)]
        for o in range(taps):
            at = EDGE - taps + 1 + o
            acc = acc + w[o:o + 1] * pre_n[c, at:at + 1, :]
        return rounded(silu(acc))

    new_values = jnp.concatenate([new_conv(c, vcol + c * part) for c in range(vparts)], axis=1)
    new_keys = new_conv(vparts, inner + gcol)
    new_query = new_conv(vparts + 1, inner + keys_all + gcol)
    gate = jnp.concatenate([pre_n[vparts + 2 + c, EDGE:EDGE + 1, :] for c in range(vparts)], axis=1)
    new_raw = rounded(lax.dot_general(
        newest, wdts[...], (((1,), (1,)), ((), ())), preferred_element_type=F32)[0:1])
    new_steps = softplus(new_raw + dtb_ref[...])
    head_s[...] = jnp.zeros_like(head_s)
    head_s[0:1, :] = new_steps
    head_s[1:2, :] = jnp.exp(-jnp.exp(alog_ref[...]) * new_steps)
    head_s[2:3, :] = dskip_ref[...]
    hrow = lax.broadcasted_iota(jnp.int32, (heads, hl * p_size), 0)
    hcol = lax.broadcasted_iota(jnp.int32, (heads, hl * p_size), 1)
    first = j * hl
    onehot = ((hcol >= (hrow - first) * p_size) & (hcol < (hrow - first + 1) * p_size)).astype(F32)
    spread_rows = jnp.dot(head_s[...], onehot, precision=lax.Precision.HIGHEST, preferred_element_type=F32)
    step_row, decay_row, skip_row = spread_rows[0:1], spread_rows[1:2], spread_rows[2:3]

    pass_on(steps - lag)
    pl.when(near)(lambda: pass_on(steps - 1))
    for g in range(gl):
        for k in range(pairs + 1):
            pltpu.make_async_remote_copy(
                src_ref=st_out.at[0, 0], dst_ref=st_in.at[k, g], send_sem=st_send.at[0, 0],
                recv_sem=st_recv.at[k, g], device_id={"sp": after, "tp": j}, device_id_type=MESH).wait_recv()
        query = new_query[:, g * n_size:(g + 1) * n_size]
        key = new_keys[:, g * n_size:(g + 1) * n_size]
        query_rows = jnp.broadcast_to(query, (EDGE, n_size)).astype(BF16)
        helds = []
        for r in range(ratio):
            h = g * ratio + r
            acc = jnp.zeros((p_size, n_size), F32)
            for k in range(pairs + 1):
                acc += st_in[k, g, r * p_size:(r + 1) * p_size, :].astype(F32)
            top = acc.astype(BF16)
            state_ref[0, h] = top
            held = jnp.zeros((EDGE, p_size), F32)
            rest = acc
            for _ in range(3):
                term = rest.astype(BF16)
                held += lax.dot_general(query_rows, term, (((1,), (1,)), ((), ())), preferred_element_type=F32)
                rest = rest - term.astype(F32)
            helds.append(held[0:1])
        span = slice(g * gcols, (g + 1) * gcols)
        held_row = jnp.concatenate(helds, axis=1)
        inner_prod = jnp.sum(query * key, axis=1, keepdims=True)
        value_row = new_values[:, span]
        out = (decay_row[:, span] * held_row + (step_row[:, span] * inner_prod) * value_row
               + skip_row[:, span] * value_row)
        gated = out * silu(gate[:, span])
        ms = jnp.sum(gated * gated, axis=1, keepdims=True) / gcols
        normed = gated * lax.rsqrt(ms + EPS)
        for r in range(ratio):
            h = g * ratio + r
            read_s[h:h + 1, :] = normed[:, r * p_size:(r + 1) * p_size] * ng_ref[h:h + 1, :]
    read_ref[0] = read_s[...].astype(BF16)

    @pl.when(i == sp - 1)
    def _():
        for a in range(spt):
            here, remote, _ = tail(a)
            pl.when(jnp.logical_not(here))(remote.wait_send)

    for q in range(tp):
        pl.when(root & (q != j))(relay(q).wait_send)
    for k in range(sp):
        pl.when(i != k)(tot(k).wait_send)
    for s in range(steps):
        for gp in range(PAIR):
            a_copy(s, gp).wait_send()
            pl.when(far)(b_copy(s, gp).wait_send)
            here, remote, _ = state_copy(s, gp)
            pl.when(jnp.logical_not(far) & jnp.logical_not(here))(remote.wait_send)


def per_device(
    dims, x_in, x_new, w_x, w_b, w_c, w_dt, w_z, conv_w, conv_b, dt_bias, a_log, d_skip, norm_g
):
    sp, tp, heads, groups, n_size, p_size, ratio, taps = dims
    spt, length, width = x_in.shape
    hl, gl = heads // tp, groups // tp
    assert x_new.shape[0] == 1 and sp == spt * tp and spt == 2 and sp % 4 == 0
    steps, gcols = groups // PAIR, ratio * p_size
    tiles = PAIR * (gcols + n_size) // LANES
    news = 2 + 2 * (hl * p_size) // (gl * n_size)
    any_spec = pl.BlockSpec(memory_space=pl.ANY)
    vmem = pl.BlockSpec(memory_space=pltpu.VMEM)
    dma = pltpu.SemaphoreType.DMA
    return pl.pallas_call(
        functools.partial(kernel, dims),
        out_shape=(
            jax.ShapeDtypeStruct((1, hl, p_size, n_size), BF16),
            jax.ShapeDtypeStruct((1, hl, p_size), BF16),
        ),
        in_specs=[any_spec, vmem] + [any_spec] * 7 + [vmem] * 4,
        out_specs=(vmem, vmem),
        scratch_shapes=[
            pltpu.VMEM((spt, EDGE + length, width), BF16),
            pltpu.VMEM((steps, width, PAIR * gcols), BF16),
            pltpu.VMEM((steps, width, PAIR * n_size), BF16),
            pltpu.VMEM((heads, width), BF16),
            pltpu.VMEM((news, width, gl * n_size), BF16),
            pltpu.VMEM((news, 2 * EDGE, gl * n_size), F32),
            pltpu.VMEM((2 * EDGE, width), BF16),
            pltpu.VMEM((tiles, EDGE + length, LANES), F32),
            pltpu.VMEM((tiles, EDGE + length, LANES), F32),
            pltpu.VMEM((length, LANES), F32),
            pltpu.VMEM((spt, heads, length), F32),
            pltpu.VMEM((8, LANES), F32),
            pltpu.VMEM((sp, 8, LANES), F32),
            pltpu.VMEM((spt, heads, LANES), F32),
            pltpu.VMEM((spt, PAIR, gcols, n_size), F32),
            pltpu.VMEM((steps, PAIR, gcols, n_size), BF16),
            pltpu.VMEM((steps, PAIR, gcols, n_size), BF16),
            pltpu.VMEM((steps, PAIR, gcols, n_size), BF16),
            pltpu.VMEM((steps, PAIR, gcols, n_size), BF16),
            pltpu.VMEM((steps, PAIR, gcols, n_size), BF16),
            pltpu.VMEM((sp // 4 + 1, gl, gcols, n_size), BF16),
            pltpu.VMEM((8, heads), F32),
            pltpu.VMEM((hl, p_size), F32),
            pltpu.VMEM(conv_w.shape, F32),
            pltpu.VMEM((1, conv_w.shape[1]), F32),
            dma((spt,)), dma, dma((steps, 2)), dma((news,)), dma((2,)), dma((spt,)), dma((spt,)),
            dma((spt,)), dma((1,)), dma((tp,)), dma((sp,)), dma((sp,)), dma((steps, PAIR)), dma((steps, PAIR)),
            dma((steps, PAIR)), dma((steps, PAIR)), dma((steps, PAIR)), dma((sp // 4 + 1, gl)),
        ],
        compiler_params=pltpu.CompilerParams(
            collective_id=0, has_side_effects=True, vmem_limit_bytes=60 * 1024 * 1024
        ),
    )(
        x_in, x_new, w_x, w_b, w_c, w_dt.T, w_z, conv_w, conv_b.reshape(1, -1),
        dt_bias.reshape(1, -1), a_log.reshape(1, -1), d_skip.reshape(1, -1), norm_g,
    )


def solution(mesh):
    sp, tp = mesh.shape["sp"], mesh.shape["tp"]

    def step(x_in, x_new, w_x, w_b, w_c, w_dt, w_z, conv_w, conv_b, dt_bias, a_log, d_skip, norm_g):
        heads, p_size = w_dt.shape[1], norm_g.shape[1]
        keys_all = w_b.shape[1]
        n_size = LANES
        groups = keys_all // n_size
        dims = (sp, tp, heads, groups, n_size, p_size, heads // groups, conv_w.shape[0])
        return per_device(
            dims, x_in, x_new, w_x, w_b, w_c, w_dt, w_z, conv_w, conv_b, dt_bias, a_log, d_skip, norm_g)

    return jax.shard_map(
        step,
        mesh=mesh,
        in_specs=(
            P("tp", "sp", None), P("sp", None), P(), P(), P(), P(), P(None, "tp"),
            P(), P(), P(), P(), P(), P("tp", None),
        ),
        out_specs=(P("sp", "tp", None, None), P("sp", "tp", None)),
        check_vma=False,
    )
```

```python
import functools

import jax
import jax.numpy as jnp
from jax import lax
from jax.experimental import pallas as pl
from jax.experimental.pallas import tpu as pltpu
from jax.sharding import PartitionSpec as P

MESH = pl.DeviceIdType.MESH
F32 = jnp.float32
BF16 = jnp.bfloat16
EPS = 1e-05
EDGE = 16
SENT = 8
PAIR = 2
LANES = 128


def silu(x):
    half = 0.5 * x
    return half + half * jnp.tanh(half)


def softplus(x):
    return jnp.maximum(x, 0.0) + jnp.log1p(jnp.exp(-jnp.abs(x)))


def rounded(x):
    return x.astype(BF16).astype(F32)


def kernel(
    dims,
    x_ref, xn_ref, wx_ref, wb_ref, wc_ref, wdt_ref, wz_ref,
    cw_hbm, cb_hbm, dtb_ref, alog_ref, dskip_ref, ng_ref,
    state_ref, read_ref,
    xs, wxs, wbs, wdts, wxn, wbn, wcn, wzn, nt, pre0, pre1, padded,
    wt, tot_out, tot_in, fcol, terms, a_out, a_in, mine, b_in, st_out, st_in, head_s, read_s, cw_ref, cb_ref,
    x_sem, wdt_sem, w_sem, new_sem, conv_sem, halo_send, halo_recv, tail_send, tail_recv, relay_send,
    tot_send, tot_recv, a_send, a_recv, b_send, b_recv, st_send, st_recv,
):
    sp, tp, heads, groups, n_size, p_size, ratio, taps = dims
    i, j = lax.axis_index("sp"), lax.axis_index("tp")
    spt, length, _ = x_ref.shape
    hl, gl = heads // tp, groups // tp
    inner, keys_all = heads * p_size, groups * n_size
    gcols = ratio * p_size
    steps = groups // PAIR
    home = i // spt
    pres = (pre0, pre1)
    member, m = lax.rem(i, 2), i // 2
    direct = m // 2 == j // 2
    near = jnp.logical_not(direct) & ((j > m) == (lax.rem(m, 2) == 1))
    far = jnp.logical_not(direct) & jnp.logical_not(near)
    partner, sibling = i + 1 - 2 * member, i + 2 - 4 * lax.rem(m, 2)
    pairs = sp // 4

    nt[0:EDGE - SENT, :] = jnp.zeros((EDGE - SENT, nt.shape[1]), BF16)
    for a in range(spt):
        xs[a, 0:EDGE - SENT, :] = jnp.zeros((EDGE - SENT, nt.shape[1]), BF16)

    barrier = pltpu.get_barrier_semaphore()
    for k in range(sp):
        @pl.when(i != k)
        def _():
            pl.semaphore_signal(barrier, inc=1, device_id={"sp": k, "tp": j}, device_id_type=MESH)

        @pl.when(home != j)
        def _():
            pl.semaphore_signal(barrier, inc=1, device_id={"sp": k, "tp": home}, device_id_type=MESH)
    after = lax.rem(i + 1, sp)

    wdt_copy = pltpu.make_async_copy(wdt_ref, wdts, wdt_sem)
    x_copies = [
        pltpu.make_async_copy(x_ref.at[a], xs.at[a, pl.ds(EDGE, length)], x_sem.at[a])
        for a in range(spt)
    ]
    w_copies = []
    for s in range(steps):
        w_copies.append((
            pltpu.make_async_copy(
                wx_ref.at[:, pl.ds(s * PAIR * gcols, PAIR * gcols)], wxs.at[s], w_sem.at[s, 0]),
            pltpu.make_async_copy(
                wb_ref.at[:, pl.ds(s * PAIR * n_size, PAIR * n_size)], wbs.at[s], w_sem.at[s, 1]),
        ))
    vcol = pl.multiple_of(j * (hl * p_size), LANES)
    gcol = pl.multiple_of(j * (gl * n_size), LANES)
    new_copies = [
        pltpu.make_async_copy(wx_ref.at[:, pl.ds(vcol, hl * p_size)], wxn, new_sem.at[0]),
        pltpu.make_async_copy(wb_ref.at[:, pl.ds(gcol, gl * n_size)], wbn, new_sem.at[1]),
        pltpu.make_async_copy(wc_ref.at[:, pl.ds(gcol, gl * n_size)], wcn, new_sem.at[2]),
        pltpu.make_async_copy(wz_ref, wzn, new_sem.at[3]),
    ]
    conv_copies = [
        pltpu.make_async_copy(cw_hbm, cw_ref, conv_sem.at[0]),
        pltpu.make_async_copy(cb_hbm, cb_ref, conv_sem.at[1]),
    ]
    wdt_copy.start()
    for c in x_copies:
        c.start()
    for pair in w_copies[:1]:
        for c in pair:
            c.start()
    for c in conv_copies:
        c.start()
    for pair in w_copies[1:]:
        for c in pair:
            c.start()
    for c in new_copies:
        c.start()

    pl.semaphore_wait(barrier, sp - 1 + spt * (tp - 1))

    def halo(a):
        return pltpu.make_async_remote_copy(
            src_ref=x_ref.at[a, pl.ds(length - SENT, SENT)],
            dst_ref=xs.at[a, pl.ds(EDGE - SENT, SENT)],
            send_sem=halo_send.at[a], recv_sem=halo_recv.at[a],
            device_id={"sp": after, "tp": j}, device_id_type=MESH)

    for a in range(spt):
        halo(a).start()

    root = home == j

    def tail(a):
        src, dst = x_ref.at[a, pl.ds(length - SENT, SENT)], nt.at[pl.ds(EDGE - SENT, SENT)]
        return spt * j + a == i, pltpu.make_async_remote_copy(
            src_ref=src, dst_ref=dst, send_sem=tail_send.at[a], recv_sem=tail_recv.at[0],
            device_id={"sp": spt * j + a, "tp": j}, device_id_type=MESH
        ), pltpu.make_async_copy(src, dst, tail_recv.at[0])

    def relay(q):
        rows = nt.at[pl.ds(EDGE - SENT, SENT)]
        return pltpu.make_async_remote_copy(
            src_ref=rows, dst_ref=rows, send_sem=relay_send.at[q], recv_sem=tail_recv.at[0],
            device_id={"sp": i, "tp": q}, device_id_type=MESH)

    @pl.when(i == sp - 1)
    def _():
        for a in range(spt):
            here, remote, local = tail(a)
            pl.when(jnp.logical_not(here))(remote.start)
            pl.when(here)(local.start)

    padded[...] = jnp.zeros_like(padded)

    def column(row):
        padded[0:1, 0:heads] = row
        return jnp.broadcast_to(padded[0:1, :], (LANES, LANES)).T[0:heads]

    rate_row = -jnp.exp(alog_ref[...])
    rates = column(rate_row)

    rows = lax.broadcasted_iota(jnp.int32, (length, length), 0)
    cols = lax.broadcasted_iota(jnp.int32, (length, length), 1)
    later = (rows > cols).astype(F32).astype(BF16)
    wdt_copy.wait()

    def tot(k):
        return pltpu.make_async_remote_copy(
            src_ref=tot_out, dst_ref=tot_in.at[i], send_sem=tot_send.at[k], recv_sem=tot_recv.at[i],
            device_id={"sp": k, "tp": j}, device_id_type=MESH)

    tot_out[...] = jnp.zeros_like(tot_out)
    for a in range(spt):
        x_copies[a].wait()
        raw = lax.dot_general(
            xs[a, EDGE:, :], wdts[...], (((1,), (1,)), ((), ())), preferred_element_type=F32)
        padded[:, 0:heads] = softplus(rounded(raw) + dtb_ref[...])
        tot_out[a:a + 1, :] = jnp.sum(padded[...], axis=0, keepdims=True)
        sizes = padded[...].T[0:heads]
        rest = jnp.zeros_like(sizes)
        left = sizes
        for _ in range(3):
            term = left.astype(BF16)
            rest += jnp.dot(term, later, preferred_element_type=F32)
            left = left - term.astype(F32)
        wt[a] = jnp.exp(rates[:, 0:1] * rest) * sizes
    tot_in[i] = tot_out[...]
    for k in range(sp):
        pl.when(i != k)(tot(k).start)

    for a in range(spt):
        halo(a).wait()
        xs[a, 0:EDGE, :] = jnp.where(i == 0, 0.0, xs[a, 0:EDGE, :].astype(F32)).astype(BF16)

    def later_factors():
        for k in range(sp):
            @pl.when(i != k)
            def _():
                pltpu.make_async_remote_copy(
                    src_ref=tot_out, dst_ref=tot_in.at[k], send_sem=tot_send.at[k], recv_sem=tot_recv.at[k],
                    device_id={"sp": k, "tp": j}, device_id_type=MESH).wait_recv()
        beyond = jnp.zeros(tot_out.shape, F32)
        for k in range(sp):
            beyond = beyond + jnp.where(k > i, tot_in[k], 0.0)
        for a in range(spt):
            fcol[a] = column(jnp.exp(rate_row * beyond[a:a + 1, 0:heads]))

    def a_copy(s):
        return pltpu.make_async_remote_copy(
            src_ref=a_out.at[s], dst_ref=a_in.at[s], send_sem=a_send.at[s], recv_sem=a_recv.at[s],
            device_id={"sp": partner, "tp": j}, device_id_type=MESH)

    def b_copy(s):
        return pltpu.make_async_remote_copy(
            src_ref=st_out.at[s], dst_ref=b_in.at[s], send_sem=b_send.at[s], recv_sem=b_recv.at[s],
            device_id={"sp": sibling, "tp": j}, device_id_type=MESH)

    slot = jnp.where(direct & (lax.rem(m, 2) == 1), pairs, m // 2)

    def state_copy(s, gp):
        g = s * PAIR + gp
        q = g // gl
        src, dst = st_out.at[s, gp], st_in.at[slot, lax.rem(g, gl)]
        sem = st_recv.at[slot, lax.rem(g, gl)]
        return (m == j) & (q == j), pltpu.make_async_remote_copy(
            src_ref=src, dst_ref=dst, send_sem=st_send.at[s, gp], recv_sem=sem,
            device_id={"sp": spt * j + member, "tp": q}, device_id_type=MESH
        ), pltpu.make_async_copy(src, dst, sem)

    def pass_on(s):
        a_copy(s).wait_recv()

        def add(*more):
            for gp in range(PAIR):
                for r in range(0, gcols, LANES):
                    total = mine[s, gp, r:r + LANES, :].astype(F32)
                    for ref in more:
                        total += ref[s, gp, r:r + LANES, :].astype(F32)
                    st_out[s, gp, r:r + LANES, :] = total.astype(BF16)

        @pl.when(near)
        def _():
            b_copy(s).wait_recv()
            add(a_in, b_in)

        @pl.when(jnp.logical_not(near))
        def _():
            add(a_in)

        @pl.when(far)
        def _():
            b_copy(s).start()

        @pl.when(jnp.logical_not(far))
        def _():
            for gp in range(PAIR):
                here, remote, local = state_copy(s, gp)
                pl.when(jnp.logical_not(here))(remote.start)
                pl.when(here)(local.start)

    lag = jnp.where(near, 2, 1)
    for c in conv_copies:
        c.wait()

    vtiles, ktiles = PAIR * gcols // LANES, PAIR * n_size // LANES
    tiles_group = gcols // LANES
    heads_tile = LANES // p_size

    def step(s, carry):
        pltpu.make_async_copy(wx_ref.at[:, pl.ds(0, PAIR * gcols)], wxs.at[s], w_sem.at[s, 0]).wait()
        pltpu.make_async_copy(wb_ref.at[:, pl.ds(0, PAIR * n_size)], wbs.at[s], w_sem.at[s, 1]).wait()

        def project(a):
            values = jnp.dot(xs[a], wxs[s], preferred_element_type=F32)
            for c in range(vtiles):
                pres[a % 2][c] = rounded(values[:, c * LANES:(c + 1) * LANES])
            keys = jnp.dot(xs[a], wbs[s], preferred_element_type=F32)
            for c in range(ktiles):
                pres[a % 2][vtiles + c] = rounded(keys[:, c * LANES:(c + 1) * LANES])

        def conv(a, c):
            if c < vtiles:
                at = pl.multiple_of(s * (PAIR * gcols) + c * LANES, LANES)
            else:
                at = pl.multiple_of(inner + s * (PAIR * n_size) + (c - vtiles) * LANES, LANES)
            acc = cb_ref[:, pl.ds(at, LANES)]
            w = cw_ref[:, pl.ds(at, LANES)]
            for o in range(taps):
                acc = acc + w[o:o + 1] * pres[a % 2][c, pl.ds(EDGE - taps + 1 + o, length), :]
            return silu(acc).astype(BF16)

        def contract(a):
            weights = wt[a, pl.ds(pl.multiple_of(s * (PAIR * ratio), PAIR * ratio), PAIR * ratio), :]
            for gp in range(PAIR):
                key = conv(a, vtiles + gp)
                parts = []
                for c in range(gp * tiles_group, (gp + 1) * tiles_group):
                    turned = conv(a, c).T
                    for r in range(heads_tile):
                        h = c * heads_tile + r
                        part = turned[r * p_size:(r + 1) * p_size].astype(F32)
                        parts.append((weights[h:h + 1] * part).astype(BF16))
                scaled = jnp.concatenate(parts, axis=0)
                terms[a, gp] = jnp.dot(scaled, key, preferred_element_type=F32)

        for a in range(spt):
            project(a)
            if a > 0:
                contract(a - 1)
        contract(spt - 1)
        pl.when(s == 0)(later_factors)
        at = pl.multiple_of(s * (PAIR * ratio), PAIR * ratio)
        factors = [fcol[a, pl.ds(at, PAIR * ratio), :] for a in range(spt)]
        for gp in range(PAIR):
            for r in range(ratio):
                h, span = gp * ratio + r, slice(r * p_size, (r + 1) * p_size)
                first, second = (factors[a][h:h + 1] * terms[a, gp, span, :] for a in range(spt))
                a_out[s, gp, span, :] = jnp.where(member == 0, second, first).astype(BF16)
                mine[s, gp, span, :] = jnp.where(member == 0, first, second).astype(BF16)
        a_copy(s).start()
        pl.when(s >= lag)(lambda: pass_on(s - lag))

        @pl.when(root & (s == steps - 1))
        def _():
            tail(0)[1].wait_recv()
            for q in range(tp):
                pl.when(q != j)(relay(q).start)

        return carry

    lax.fori_loop(0, steps, step, 0)

    newest = jnp.broadcast_to(xn_ref[...].astype(F32), (EDGE, xn_ref.shape[1])).astype(BF16)
    nt[EDGE:2 * EDGE, :] = newest
    pl.when(jnp.logical_not(root))(tail(0)[1].wait_recv)
    for c in new_copies:
        c.wait()

    def new_conv(w_ref, start, width):
        pre = rounded(jnp.dot(nt[...], w_ref[...], preferred_element_type=F32))
        start = pl.multiple_of(start, LANES)
        acc = cb_ref[:, pl.ds(start, width)]
        w = cw_ref[:, pl.ds(start, width)]
        for o in range(taps):
            at = EDGE - taps + 1 + o
            acc = acc + w[o:o + 1] * pre[at:at + 1]
        return rounded(silu(acc))

    new_values = new_conv(wxn, vcol, hl * p_size)
    new_keys = new_conv(wbn, inner + gcol, gl * n_size)
    new_query = new_conv(wcn, inner + keys_all + gcol, gl * n_size)
    gate = rounded(jnp.dot(newest, wzn[...], preferred_element_type=F32)[0:1])
    new_raw = rounded(lax.dot_general(
        newest, wdts[...], (((1,), (1,)), ((), ())), preferred_element_type=F32)[0:1])
    new_steps = softplus(new_raw + dtb_ref[...])
    head_s[...] = jnp.zeros_like(head_s)
    head_s[0:1, :] = new_steps
    head_s[1:2, :] = jnp.exp(-jnp.exp(alog_ref[...]) * new_steps)
    head_s[2:3, :] = dskip_ref[...]
    hrow = lax.broadcasted_iota(jnp.int32, (heads, hl * p_size), 0)
    hcol = lax.broadcasted_iota(jnp.int32, (heads, hl * p_size), 1)
    first = j * hl
    onehot = ((hcol >= (hrow - first) * p_size) & (hcol < (hrow - first + 1) * p_size)).astype(F32)
    spread_rows = jnp.dot(head_s[...], onehot, precision=lax.Precision.HIGHEST, preferred_element_type=F32)
    step_row, decay_row, skip_row = spread_rows[0:1], spread_rows[1:2], spread_rows[2:3]

    pass_on(steps - lag)
    pl.when(near)(lambda: pass_on(steps - 1))
    for g in range(gl):
        for k in range(pairs + 1):
            pltpu.make_async_remote_copy(
                src_ref=st_out.at[0, 0], dst_ref=st_in.at[k, g], send_sem=st_send.at[0, 0],
                recv_sem=st_recv.at[k, g], device_id={"sp": after, "tp": j}, device_id_type=MESH).wait_recv()
        query = new_query[:, g * n_size:(g + 1) * n_size]
        key = new_keys[:, g * n_size:(g + 1) * n_size]
        query_rows = jnp.broadcast_to(query, (EDGE, n_size)).astype(BF16)
        helds = []
        for r in range(ratio):
            h = g * ratio + r
            acc = jnp.zeros((p_size, n_size), F32)
            for k in range(pairs + 1):
                acc += st_in[k, g, r * p_size:(r + 1) * p_size, :].astype(F32)
            top = acc.astype(BF16)
            state_ref[0, h] = top
            held = jnp.zeros((EDGE, p_size), F32)
            rest = acc
            for _ in range(3):
                term = rest.astype(BF16)
                held += lax.dot_general(query_rows, term, (((1,), (1,)), ((), ())), preferred_element_type=F32)
                rest = rest - term.astype(F32)
            helds.append(held[0:1])
        span = slice(g * gcols, (g + 1) * gcols)
        held_row = jnp.concatenate(helds, axis=1)
        inner_prod = jnp.sum(query * key, axis=1, keepdims=True)
        value_row = new_values[:, span]
        out = (decay_row[:, span] * held_row + (step_row[:, span] * inner_prod) * value_row
               + skip_row[:, span] * value_row)
        gated = out * silu(gate[:, span])
        ms = jnp.sum(gated * gated, axis=1, keepdims=True) / gcols
        normed = gated * lax.rsqrt(ms + EPS)
        for r in range(ratio):
            h = g * ratio + r
            read_s[h:h + 1, :] = normed[:, r * p_size:(r + 1) * p_size] * ng_ref[h:h + 1, :]
    read_ref[0] = read_s[...].astype(BF16)

    @pl.when(i == sp - 1)
    def _():
        for a in range(spt):
            here, remote, _ = tail(a)
            pl.when(jnp.logical_not(here))(remote.wait_send)

    for q in range(tp):
        pl.when(root & (q != j))(relay(q).wait_send)
    for k in range(sp):
        pl.when(i != k)(tot(k).wait_send)
    for s in range(steps):
        a_copy(s).wait_send()
        pl.when(far)(b_copy(s).wait_send)
        for gp in range(PAIR):
            here, remote, _ = state_copy(s, gp)
            pl.when(jnp.logical_not(far) & jnp.logical_not(here))(remote.wait_send)


def hand_over(state_in, read_in, state_out, read_out):
    state_out[...] = state_in[...]
    read_out[...] = read_in[...]


def per_device(
    dims, x_in, x_new, w_x, w_b, w_c, w_dt, w_z, conv_w, conv_b, dt_bias, a_log, d_skip, norm_g
):
    sp, tp, heads, groups, n_size, p_size, ratio, taps = dims
    spt, length, width = x_in.shape
    hl, gl = heads // tp, groups // tp
    assert x_new.shape[0] == 1 and sp == spt * tp and spt == 2 and sp % 4 == 0
    steps, gcols = groups // PAIR, ratio * p_size
    tiles = PAIR * (gcols + n_size) // LANES
    any_spec = pl.BlockSpec(memory_space=pl.ANY)
    vmem = pl.BlockSpec(memory_space=pltpu.VMEM)
    dma = pltpu.SemaphoreType.DMA
    results = pl.pallas_call(
        functools.partial(kernel, dims),
        out_shape=(
            jax.ShapeDtypeStruct((1, hl, p_size, n_size), BF16),
            jax.ShapeDtypeStruct((1, hl, p_size), BF16),
        ),
        in_specs=[any_spec, vmem] + [any_spec] * 7 + [vmem] * 4,
        out_specs=(vmem, vmem),
        scratch_shapes=[
            pltpu.VMEM((spt, EDGE + length, width), BF16),
            pltpu.VMEM((steps, width, PAIR * gcols), BF16),
            pltpu.VMEM((steps, width, PAIR * n_size), BF16),
            pltpu.VMEM((heads, width), BF16),
            pltpu.VMEM((width, hl * p_size), BF16),
            pltpu.VMEM((width, gl * n_size), BF16),
            pltpu.VMEM((width, gl * n_size), BF16),
            pltpu.VMEM((width, hl * p_size), BF16),
            pltpu.VMEM((2 * EDGE, width), BF16),
            pltpu.VMEM((tiles, EDGE + length, LANES), F32),
            pltpu.VMEM((tiles, EDGE + length, LANES), F32),
            pltpu.VMEM((length, LANES), F32),
            pltpu.VMEM((spt, heads, length), F32),
            pltpu.VMEM((8, LANES), F32),
            pltpu.VMEM((sp, 8, LANES), F32),
            pltpu.VMEM((spt, heads, LANES), F32),
            pltpu.VMEM((spt, PAIR, gcols, n_size), F32),
            pltpu.VMEM((steps, PAIR, gcols, n_size), BF16),
            pltpu.VMEM((steps, PAIR, gcols, n_size), BF16),
            pltpu.VMEM((steps, PAIR, gcols, n_size), BF16),
            pltpu.VMEM((steps, PAIR, gcols, n_size), BF16),
            pltpu.VMEM((steps, PAIR, gcols, n_size), BF16),
            pltpu.VMEM((sp // 4 + 1, gl, gcols, n_size), BF16),
            pltpu.VMEM((8, heads), F32),
            pltpu.VMEM((hl, p_size), F32),
            pltpu.VMEM(conv_w.shape, F32),
            pltpu.VMEM((1, conv_w.shape[1]), F32),
            dma((spt,)), dma, dma((steps, 2)), dma((4,)), dma((2,)), dma((spt,)), dma((spt,)),
            dma((spt,)), dma((1,)), dma((tp,)), dma((sp,)), dma((sp,)), dma((steps,)), dma((steps,)),
            dma((steps,)), dma((steps,)), dma((steps, PAIR)), dma((sp // 4 + 1, gl)),
        ],
        compiler_params=pltpu.CompilerParams(
            collective_id=0, has_side_effects=True, vmem_limit_bytes=60 * 1024 * 1024
        ),
    )(
        x_in, x_new, w_x, w_b, w_c, w_dt.T, w_z, conv_w, conv_b.reshape(1, -1),
        dt_bias.reshape(1, -1), a_log.reshape(1, -1), d_skip.reshape(1, -1), norm_g,
    )
    return pl.pallas_call(
        hand_over,
        out_shape=tuple(jax.ShapeDtypeStruct(r.shape, r.dtype) for r in results),
        in_specs=[vmem, vmem],
        out_specs=(vmem, vmem),
        compiler_params=pltpu.CompilerParams(vmem_limit_bytes=4 * 1024 * 1024),
    )(*results)


def solution(mesh):
    sp, tp = mesh.shape["sp"], mesh.shape["tp"]

    def step(x_in, x_new, w_x, w_b, w_c, w_dt, w_z, conv_w, conv_b, dt_bias, a_log, d_skip, norm_g):
        heads, p_size = w_dt.shape[1], norm_g.shape[1]
        keys_all = w_b.shape[1]
        n_size = LANES
        groups = keys_all // n_size
        dims = (sp, tp, heads, groups, n_size, p_size, heads // groups, conv_w.shape[0])
        return per_device(
            dims, x_in, x_new, w_x, w_b, w_c, w_dt, w_z, conv_w, conv_b, dt_bias, a_log, d_skip, norm_g)

    return jax.shard_map(
        step,
        mesh=mesh,
        in_specs=(
            P("tp", "sp", None), P("sp", None), P(), P(), P(), P(), P(None, "tp"),
            P(), P(), P(), P(), P(), P("tp", None),
        ),
        out_specs=(P("sp", "tp", None, None), P("sp", "tp", None)),
        check_vma=False,
    )
```
